256 devices in a mesh: ep: 16 (over y, x), tp: 16 (over z, core).
Axes of the slice: x: 4, y: 4, z: 8, core: 2. Of those that a mesh axis runs over, the one named last changes fastest.
Arguments:
- mixer_in: bfloat16 [32768, 2048], P(('ep', 'tp')), may hold values from -6 to 6
- expert_in: bfloat16 [32768, 2048], P(('ep', 'tp')), may hold values from -6 to 6
- mixer_gain: float32 [2048], replicated, may hold values from 0.1 to 1.9
- w_outer: bfloat16 [2048, 2048], P(None, 'tp'), may hold values from -0.125 to 0.125
- w_inner: bfloat16 [2048, 2048], P(None, 'tp'), may hold values from -0.125 to 0.125
- w_value: bfloat16 [2048, 2048], P(None, 'tp'), may hold values from -0.125 to 0.125
- conv_taps: float32 [3, 2048], P(None, 'tp'), may hold values from -3 to 3
- w_mix_out: bfloat16 [2048, 2048], P('tp'), may hold values from -0.125 to 0.125
- expert_gain: float32 [2048], replicated, may hold values from 0.1 to 1.9
- w_gate: bfloat16 [32, 2048, 2048], P('ep', None, 'tp'), may hold values from -0.375 to 0.375
- w_up: bfloat16 [32, 2048, 2048], P('ep', None, 'tp'), may hold values from -0.375 to 0.375
- w_down: bfloat16 [32, 2048, 2048], P('ep', 'tp'), may hold values from -0.02734375 to 0.02734375
- route_ids: int32 [32768, 2], P(('ep', 'tp')), may hold values from 0 to 31, all different within a row; in each aligned block of 128 rows (0 to 127, 128 to 255, ...) at most 10 rows name the same one
- route_weights: float32 [32768, 2], P(('ep', 'tp')), may hold values from 0.2 to 1
Outputs:
- mixer_out: bfloat16 [32768, 2048], P(('ep', 'tp'))
- expert_out: bfloat16 [32768, 2048], P(('ep', 'tp'))
The draws below stay inside these ranges and needn't reach their ends.
Inputs may be any that keep to these rules, and one draw needn't show every extreme that they name: `route_ids`: each row names 2 different experts. Among the 128 rows of one device no expert is named more than 10 times, and in every draw some device names some expert exactly 10 times.
All inputs are finite; a program needn't handle non-finite values.
Results may differ from the reference program's by a relative error of at most 0.019.
Values may be sent and summed in bfloat16 or wider, within the bound.
A program may use at most 128 MiB of HBM per device.

```python
import math
import jax
import jax.numpy as jnp
import numpy as np
from jax import lax

D = 2048
FF = 2048
EXPERTS = 32
TOP = 2
CONV = 3
ROWS = 128
CAP = 10
TOKENS = 32768
N_TP = 16


def level_of(rng, shape, pieces, low, high):
    factor_of, own = 1.0, jax.random.fold_in(rng, 6)
    for axis_at, shards_of in pieces:
        steps = jnp.exp(jax.random.uniform(jax.random.fold_in(own, axis_at), (shards_of,), jnp.float32, low / len(pieces), high / len(pieces)))
        factor_of = factor_of * jnp.repeat(steps, shape[axis_at] // shards_of).reshape([-1 if axis == axis_at else 1 for axis in range(len(shape))])
    return factor_of


def shared_out(own_key, own, number, rows, number_of, top, reach, skew):
    order = jax.random.permutation(own_key, number_of)
    crowded, common = load_shares(number_of, rows * top, reach, skew, True), load_shares(number_of, rows * top, reach, skew, False)
    places = jnp.arange(number_of)

    def named(sizes, turn):
        used = int((sizes > 0).sum())
        fixed = max(1, used // 4)
        shifted = fixed + (places - fixed + turn * (used - fixed)) % max(1, number_of - fixed)
        return jnp.zeros((number_of,), jnp.int32).at[order[jnp.where(places < fixed, places, shifted)]].set(jnp.asarray(sizes, jnp.int32))

    sizes = jnp.where(number % 4 == 0, named(crowded, number // 4), named(common, number - number // 4 - 1))
    mixed = jax.random.permutation(jax.random.fold_in(own, 3), number_of)
    source_of, sink = mixed[0:number_of // 2 * 2:2], mixed[1:number_of // 2 * 2:2]
    margin = jnp.minimum(sizes[source_of] - 1, reach - sizes[sink]) // 2
    margin = jnp.where((source_of == order[0]) | (sink == order[0]) | (sizes[sink] == 0), 0, jnp.maximum(margin, 0))
    shifted = jax.random.randint(jax.random.fold_in(own, 4), (number_of // 2,), 0, 1 << 20) % (margin + 1)
    sizes = sizes.at[source_of].add(-shifted).at[sink].add(shifted)
    labels = jnp.searchsorted(jnp.cumsum(sizes), jnp.arange(rows * top), side="right").astype(jnp.int32)
    table = labels.reshape(top, rows).T
    table = table[jax.random.permutation(jax.random.fold_in(own, 1), rows)]
    turn = jax.random.randint(jax.random.fold_in(own, 2), (rows, 1), 0, top)
    return jnp.take_along_axis(table, (jnp.arange(top)[None, :] + turn) % top, axis=1)


def load_shares(amount, total, bound, slope, full):
    portions = [(1 << 20) // math.isqrt(standing ** slope) + 1 for standing in range(1, amount + 1)]
    largest = bound if full else min(bound, max(-(-total // amount), total * portions[0] // sum(portions)))
    least = 1 if total - largest >= amount - 1 else 0
    given, rest = [largest] + [least] * (amount - 1), total - largest - least * (amount - 1)
    while rest > 0:
        free = [i for i in range(1, amount) if given[i] < largest] or [i for i in range(1, amount) if given[i] < bound]
        mass, remaining = sum([portions[i] for i in free]), rest
        for i in free:
            addition = min(bound - given[i], max(1, remaining * portions[i] // mass), rest)
            given[i] = given[i] + addition
            rest = rest - addition
    return np.array(given)


def noise(stream_key, extent, spread, most, shards=(), kind=jnp.bfloat16):
    result = jax.random.normal(stream_key, extent, jnp.float32) * spread
    if len(shards) > 0:
        result = level_of(stream_key, extent, shards, -0.22, 0.18) * result
    return jnp.clip(result, min=-most, max=most).astype(kind)


def setup_inputs(seed: int = 0) -> dict:
    keys = jax.random.split(jax.random.key(seed), 15)
    mixer_in = noise(keys[0], (TOKENS, D), 1.0, 6.0, ((0, 256),))
    expert_in = noise(keys[1], (TOKENS, D), 1.0, 6.0, ((0, 256),))
    mixer_gain = jnp.clip(1.0 + 0.18 * jax.random.normal(keys[2], (D,), jnp.float32), 0.1, 1.9)
    w_outer = noise(keys[3], (D, D), D ** -0.5, 0.125, ((1, 16),))
    w_inner = noise(keys[4], (D, D), D ** -0.5, 0.125, ((1, 16),))
    w_value = noise(keys[5], (D, D), D ** -0.5, 0.125, ((1, 16),))
    conv_taps = noise(keys[6], (CONV, D), 0.6, 3.0, ((1, 16),), jnp.float32)
    w_mix_out = noise(keys[7], (D, D), D ** -0.5, 0.125, ((0, 16),))
    expert_gain = jnp.clip(1.0 + 0.18 * jax.random.normal(keys[8], (D,), jnp.float32), 0.1, 1.9)
    w_gate = noise(keys[9], (EXPERTS, D, FF), (D // 9) ** -0.5, 0.375, ((0, 16), (2, 16)))
    w_up = noise(keys[10], (EXPERTS, D, FF), (D // 9) ** -0.5, 0.375, ((0, 16), (2, 16)))
    w_down = noise(keys[11], (EXPERTS, FF, D), (FF * 25) ** -0.5, 0.02734375, ((0, 16), (1, 16)))
    route_ids_keys = jax.random.split(jax.random.fold_in(keys[12], 1), TOKENS // ROWS)
    route_ids_turns = jax.random.permutation(jax.random.fold_in(keys[12], 3), TOKENS // ROWS)
    route_ids = jax.vmap(lambda own, number: shared_out(jax.random.fold_in(keys[12], 2), own, number, ROWS, EXPERTS, TOP, CAP, 2))(route_ids_keys, route_ids_turns).reshape((TOKENS, TOP))
    route_weights = jnp.clip(jnp.exp(math.log(1.0) - 1.609438 * jax.random.uniform(keys[13], (TOKENS, TOP), jnp.float32) ** level_of(keys[13], (TOKENS, TOP), ((0, 256),), -0.2, 0.2)), 0.2, 1.0)
    return dict(mixer_in=mixer_in, expert_in=expert_in, mixer_gain=mixer_gain, w_outer=w_outer, w_inner=w_inner, w_value=w_value, conv_taps=conv_taps, w_mix_out=w_mix_out, expert_gain=expert_gain, w_gate=w_gate, w_up=w_up, w_down=w_down, route_ids=route_ids, route_weights=route_weights)


norm_eps = 1e-06
clamp_limit = 7.0
gate_alpha = 1.702

def rms_scale(tok_rows, gain_vec):
    values = tok_rows.astype(jnp.float32)
    scaled = values * lax.rsqrt(lax.optimization_barrier(jnp.mean(values * values, axis=-1, keepdims=True)) + norm_eps)
    return (scaled * gain_vec.astype(jnp.float32)).astype(jnp.bfloat16)

def grouped_product(left_rows, right_rows):
    slice_width = left_rows.shape[1] // N_TP
    running = jnp.zeros((left_rows.shape[0], right_rows.shape[1]), jnp.float32)
    for shard_index in range(N_TP):
        lower = shard_index * slice_width
        piece_sum = jnp.dot(left_rows[:, lower:lower + slice_width], right_rows[lower:lower + slice_width], preferred_element_type=jnp.float32).astype(jnp.bfloat16)
        running = running + lax.optimization_barrier(piece_sum).astype(jnp.float32)
    return running

def reference(mixer_in, expert_in, mixer_gain, w_outer, w_inner, w_value, conv_taps, w_mix_out, expert_gain, w_gate, w_up, w_down, route_ids, route_weights):
    normed_mix = rms_scale(mixer_in, mixer_gain)
    outer_gate = jnp.dot(normed_mix, w_outer, preferred_element_type=jnp.float32)
    inner_prod = jnp.dot(normed_mix, w_inner, preferred_element_type=jnp.float32) * jnp.dot(normed_mix, w_value, preferred_element_type=jnp.float32)
    padded = jnp.pad(inner_prod, ((2, 0), (0, 0)))
    conv_out = conv_taps[2] * inner_prod + conv_taps[1] * padded[1:TOKENS + 1] + conv_taps[0] * padded[:TOKENS]
    gated_rows = (outer_gate * conv_out).astype(jnp.bfloat16)
    mixer_out = grouped_product(gated_rows, w_mix_out).astype(jnp.bfloat16)
    normed_exp = rms_scale(expert_in, expert_gain)
    blocks = TOKENS // ROWS
    block_ids = route_ids.reshape(blocks, ROWS * TOP).astype(jnp.int32)
    member = (block_ids[:, :, None] == jnp.arange(EXPERTS, dtype=jnp.int32)[None, None, :]).astype(jnp.int32)
    earlier = jnp.cumsum(member, axis=1) - member
    slot_in = lax.optimization_barrier(jnp.sum(earlier * member, axis=2))
    flat_pos = block_ids * (blocks * CAP) + jnp.arange(blocks, dtype=jnp.int32)[:, None] * CAP + slot_in
    flat_pos = flat_pos.reshape(-1).astype(jnp.int32)
    owner_rows = jnp.repeat(jnp.arange(TOKENS, dtype=jnp.int32), TOP)
    buffer = jnp.zeros((EXPERTS * blocks * CAP, D), jnp.bfloat16).at[flat_pos].set(normed_exp[owner_rows])
    buffer = buffer.reshape(EXPERTS, blocks * CAP, D)

    def one_expert(inputs):
        slot_rows, gate_w, up_w, down_w = inputs
        gate_pre = jnp.minimum(jnp.dot(slot_rows, gate_w, preferred_element_type=jnp.float32), clamp_limit)
        up_pre = jnp.clip(jnp.dot(slot_rows, up_w, preferred_element_type=jnp.float32), -clamp_limit, clamp_limit)
        hidden = ((up_pre + 1.0) * gate_pre * jax.nn.sigmoid(gate_alpha * gate_pre)).astype(jnp.bfloat16)
        return grouped_product(hidden, down_w).astype(jnp.bfloat16)
    outputs = lax.map(one_expert, (buffer, w_gate, w_up, w_down))
    picked = outputs.reshape(-1, D)[flat_pos].reshape(TOKENS, TOP, D)
    expert_out = lax.optimization_barrier(jnp.sum(picked.astype(jnp.float32) * route_weights.astype(jnp.float32)[:, :, None], axis=1)).astype(jnp.bfloat16)
    return (mixer_out, expert_out)
```

```python
import functools

import jax
import jax.numpy as jnp
from jax import lax
from jax.experimental import pallas as pl
from jax.experimental.pallas import tpu as pltpu
from jax.sharding import Mesh
from jax.sharding import PartitionSpec as P

EXPERTS = 32
CAP = 10
PAD = 16
EP = 16
NZ = 8
LOCAL = 2
ROWS = EP * CAP
TP = ("tp_0", "tp_1")
EP_TP = ("ep", "tp_0", "tp_1")
MESH = pl.DeviceIdType.MESH
F32 = jnp.float32
BF16 = jnp.bfloat16

norm_eps = 1e-06
clamp_limit = 7.0
gate_alpha = 1.702


def rms_scale(tok_rows, gain_vec):
    values = tok_rows.astype(F32)
    scaled = values * lax.rsqrt(jnp.mean(values * values, axis=-1, keepdims=True) + norm_eps)
    return (scaled * gain_vec).astype(BF16)


def places():
    return lax.axis_index("ep"), lax.axis_index("tp_0"), lax.axis_index("tp_1")


def greet(ep, z, core):
    barrier = pltpu.get_barrier_semaphore()

    def one(k, _):
        pl.semaphore_signal(
            barrier, inc=1, device_id=(lax.rem(ep + k, EP), z, core), device_id_type=MESH
        )
        return 0

    lax.fori_loop(1, EP, one, 0)
    for step in (1, NZ - 1):
        pl.semaphore_signal(
            barrier, inc=1, device_id=(ep, lax.rem(z + step, NZ), core), device_id_type=MESH
        )
    pl.semaphore_signal(barrier, inc=1, device_id=(ep, z, 1 - core), device_id_type=MESH)
    pl.semaphore_wait(barrier, EP + 2)


def remote(src, dst, send, recv, where):
    return pltpu.make_async_remote_copy(
        src_ref=src, dst_ref=dst, send_sem=send, recv_sem=recv, device_id=where, device_id_type=MESH
    )


GATHER_D = (1, 1, 2, 2, 3, 3, 4)
GATHER_X = ((0, 1, 0, 1, 0, 1, 0), (0, 1, 0, 1, 0, 1, 1))
SCATTER_D = (4, 3, 3, 2, 2, 1, 1)
SCATTER_X = ((0, 1, 0, 1, 0, 1, 0), (1, 0, 1, 0, 1, 1, 0))
SCATTER_IN = ((None, None, 0, 1, 2, 3, 4), (None, None, 0, 1, 2, 4, 3))
LAST_IN = {1: (5, 5), 0: (6, 6)}
STEPS = 7


def gather_kernel(
    slots, w_gate, w_up, hid,
    units, landed, w_both,
    w_sem, a_send, a_recv, r_send, r_recv, c_send, c_recv,
):
    ep, z, core = places()
    loads = []
    for x in range(LOCAL):
        loads.append(pltpu.make_async_copy(w_gate.at[x], w_both.at[x, :, 0:128], w_sem.at[x, 0]))
        loads.append(pltpu.make_async_copy(w_up.at[x], w_both.at[x, :, 128:256], w_sem.at[x, 1]))
    for load in loads:
        load.start()
    greet(ep, z, core)

    def exchange(x, k):
        to = lax.rem(ep + k, EP)
        return remote(
            slots.at[x, to], landed.at[x, ep], a_send.at[x, k], a_recv.at[x, k], (to, z, core)
        )

    for x in range(LOCAL):

        def send_one(k, _, x=x):
            exchange(x, k).start()
            return 0

        lax.fori_loop(1, EP, send_one, 0)
    for load in loads:
        load.wait()
    for x in range(LOCAL):
        landed[x, ep] = slots[x, ep]

    row = lax.broadcasted_iota(jnp.int32, (ROWS, EP * PAD), 0)
    col = lax.broadcasted_iota(jnp.int32, (ROWS, EP * PAD), 1)
    picks = ((row // CAP) * PAD + row % CAP == col).astype(BF16)

    def compute(at_z, at_core, x):
        tok = units[at_z, at_core, x]
        both = jnp.dot(tok, w_both[x], preferred_element_type=F32)
        gate_pre = jnp.minimum(both[:, 0:128], clamp_limit)
        up_pre = jnp.clip(both[:, 128:256], -clamp_limit, clamp_limit)
        hid[at_z, at_core, x] = (
            (up_pre + 1.0) * gate_pre * jax.nn.sigmoid(gate_alpha * gate_pre)
        ).astype(BF16)

    steps = (NZ - 1, 1)

    def ring_copy(way, n):
        at = lax.rem(z + (GATHER_D[n] - 1) * steps[way], NZ)
        x = GATHER_X[way][n]
        there = lax.rem(z + (NZ - steps[way]), NZ)
        return remote(
            units.at[at, core, x], units.at[at, core, x],
            r_send.at[way, n], r_recv.at[way, n], (ep, there, core),
        )

    def across(way, n):
        at = z if n == STEPS else lax.rem(z + GATHER_D[n] * steps[way], NZ)
        x = way if n == STEPS else GATHER_X[way][n]
        ref = units.at[at, core, x]
        return remote(ref, ref, c_send.at[way, n], c_recv.at[way, n], (ep, z, 1 - core)), at, x

    for x in range(LOCAL):

        def wait_one(k, _, x=x):
            exchange(x, k).wait_recv()
            return 0

        lax.fori_loop(1, EP, wait_one, 0)

        def pack(j, _, x=x):
            cols = pl.ds(pl.multiple_of(j * 512, 512), 512)
            src = landed[x, :, :, cols].reshape(EP * PAD, 512)
            units[z, core, x, :, cols] = jnp.dot(picks, src, preferred_element_type=F32).astype(BF16)
            return 0

        lax.fori_loop(0, 4, pack, 0)
        for way in range(2):
            ring_copy(way, x).start()
        across(x, STEPS)[0].start()
    for x in range(LOCAL):
        compute(z, core, x)

    for n in range(STEPS):
        for way in range(2):
            ring_copy(way, n).wait_recv()
            nxt = 6 if (way, n) == (1, 5) else n + 2
            if nxt < STEPS and GATHER_X[way][nxt] == GATHER_X[way][n] and GATHER_D[nxt] == GATHER_D[n] + 1:
                ring_copy(way, nxt).start()
            across(way, n)[0].start()
        for way in range(2):
            at = lax.rem(z + GATHER_D[n] * steps[way], NZ)
            compute(at, core, GATHER_X[way][n])
        for way in range(2):
            copy, at, x = across(way, STEPS if n == 0 else n - 1)
            copy.wait_recv()
            compute(at, 1 - core, x)
    for way in range(2):
        copy, at, x = across(way, STEPS - 1)
        copy.wait_recv()
        compute(at, 1 - core, x)
    for way in range(2):
        for n in range(STEPS):
            ring_copy(way, n).wait_send()
            across(way, n)[0].wait_send()
        across(way, STEPS)[0].wait_send()
    for x in range(LOCAL):

        def done_one(k, _, x=x):
            exchange(x, k).wait_send()
            return 0

        lax.fori_loop(1, EP, done_one, 0)


def scatter_kernel(
    hid, w_down, back,
    c_out, c_in, r_out, r_in, b_out,
    c_send, c_recv, r_send, r_recv, a_send, a_recv,
):
    ep, z, core = places()
    greet(ep, z, core)
    steps = (1, NZ - 1)

    def place(way, m):
        if m == STEPS:
            return z, way
        return lax.rem(z + SCATTER_D[m] * steps[way], NZ), SCATTER_X[way][m]

    def across(way, m):
        return remote(
            c_out.at[way, m], c_in.at[way, m], c_send.at[way, m], c_recv.at[way, m],
            (ep, z, 1 - core),
        )

    def ring_copy(way, m):
        return remote(
            r_out.at[way, m], r_in.at[way, m], r_send.at[way, m], r_recv.at[way, m],
            (ep, lax.rem(z + steps[way], NZ), core),
        )

    def partial(at, at_core, x, add, out):
        def tile(j, _):
            cols = pl.ds(pl.multiple_of(j * 512, 512), 512)
            total = jnp.dot(hid[at, at_core, x], w_down[x, :, cols], preferred_element_type=F32)
            for ref in add:
                total = total + ref[:, cols].astype(F32)
            out[:, cols] = total.astype(BF16)
            return 0

        lax.fori_loop(0, 4, tile, 0)

    def help_other(m):
        for way in range(2):
            at, x = place(way, m)
            partial(at, 1 - core, x, (), c_out.at[way, m])
            across(way, m).start()

    help_other(0)
    help_other(1)
    for m in range(STEPS):
        for way in range(2):
            at, x = place(way, m)
            add = [c_in.at[way, m]]
            across(way, m).wait_recv()
            came = SCATTER_IN[way][m]
            if came is not None:
                ring_copy(way, came).wait_recv()
                add.append(r_in.at[way, came])
            partial(at, core, x, add, r_out.at[way, m])
            ring_copy(way, m).start()
        if m + 2 <= STEPS:
            help_other(m + 2)

    row = lax.broadcasted_iota(jnp.int32, (EP * PAD, ROWS), 0)
    col = lax.broadcasted_iota(jnp.int32, (EP * PAD, ROWS), 1)
    spread = ((row // PAD) * CAP + row % PAD == col) & (row % PAD < CAP)
    spread = spread.astype(BF16)

    def exchange(x, k):
        to = lax.rem(ep + k, EP)
        return remote(
            b_out.at[x, to], back.at[x, ep], a_send.at[x, k], a_recv.at[x, k], (to, z, core)
        )

    for x in (1, 0):
        across(x, STEPS).wait_recv()
        for way in range(2):
            ring_copy(way, LAST_IN[x][way]).wait_recv()

        def tile(j, _, x=x):
            cols = pl.ds(pl.multiple_of(j * 512, 512), 512)
            total = jnp.dot(hid[z, core, x], w_down[x, :, cols], preferred_element_type=F32)
            for ref in (c_in.at[x, STEPS], r_in.at[0, LAST_IN[x][0]], r_in.at[1, LAST_IN[x][1]]):
                total = total + ref[:, cols].astype(F32)
            wide = jnp.dot(spread, total.astype(BF16), preferred_element_type=F32).astype(BF16)
            b_out[x, :, :, cols] = wide.reshape(EP, PAD, 512)
            return 0

        lax.fori_loop(0, 4, tile, 0)

        def send_one(k, _, x=x):
            exchange(x, k).start()
            return 0

        lax.fori_loop(1, EP, send_one, 0)
        back[x, ep] = b_out[x, ep]
    for way in range(2):
        for m in range(STEPS):
            ring_copy(way, m).wait_send()
            across(way, m).wait_send()
        across(way, STEPS).wait_send()
    for x in (1, 0):

        def end_one(k, _, x=x):
            exchange(x, k).wait()
            return 0

        lax.fori_loop(1, EP, end_one, 0)


def mixer_kernel(tok, taps, blocks, out, total):
    step = pl.program_id(0)

    @pl.when(step == 0)
    def _():
        total[...] = jnp.zeros_like(total)

    rows = tok[...]
    outer, inner, value = (
        jnp.dot(rows, blocks[:, 0, 0, i].reshape(2048, 128), preferred_element_type=F32)
        for i in range(3)
    )
    prod = inner * value
    conv = taps[2:3] * prod[16:144] + taps[1:2] * prod[15:143] + taps[0:1] * prod[14:142]
    gated = (outer[16:144] * conv).astype(BF16)
    for e in range(EP):
        cols = slice(e * 128, (e + 1) * 128)
        total[:, cols] += jnp.dot(gated, blocks[e, 0, 0, 3], preferred_element_type=F32)

    @pl.when(step == pl.num_programs(0) - 1)
    def _():
        out[...] = total[...].astype(BF16)


def slot_index(route_ids, experts, capacity):
    flat_ids = route_ids.reshape(-1)
    member = (flat_ids[:, None] == jnp.arange(experts, dtype=jnp.int32)[None, :]).astype(jnp.int32)
    earlier = jnp.cumsum(member, axis=0) - member
    place = jnp.sum(earlier * member, axis=1)
    return (flat_ids % LOCAL) * (EP * PAD) + (flat_ids // LOCAL) * PAD + place


DMA = pltpu.SemaphoreType.DMA


def per_device(
    mixer_in, expert_in, mixer_gain, w_outer, w_inner, w_value, conv_taps, w_mix_out,
    expert_gain, w_gate, w_up, w_down, route_ids, route_weights,
):
    tok_count, width = expert_in.shape
    ep, z, core = places()

    part = jnp.stack(
        [lax.dynamic_slice_in_dim(w, ep * 128, 128, 0) for w in (w_outer, w_inner, w_value)]
        + [lax.dynamic_slice_in_dim(w_mix_out, ep * 128, 128, 1)]
    )
    part = lax.all_gather(part, "tp_0", axis=0, tiled=False)
    blocks = lax.all_gather(part, ("ep", "tp_1"), axis=0, tiled=False)
    blocks = blocks.reshape(EP, 2, NZ, 4, 128, 128)
    taps = lax.all_gather(conv_taps, TP, axis=0, tiled=False)

    normed_mix = rms_scale(mixer_in, mixer_gain)
    count = EP * NZ * 2
    before = lax.ppermute(normed_mix[tok_count - 16 :], EP_TP, [(i, i + 1) for i in range(count - 1)])
    mix_rows = jnp.concatenate((before, normed_mix), axis=0)

    normed_exp = rms_scale(expert_in, expert_gain)
    slot_ids = slot_index(route_ids, EXPERTS, CAP).reshape(tok_count, 2)
    wide = LOCAL * EP * PAD
    every = jnp.arange(wide, dtype=jnp.int32)
    placing = (every[:, None] == slot_ids[None, :, 0]) | (every[:, None] == slot_ids[None, :, 1])
    slots = jnp.dot(placing.astype(BF16), normed_exp, preferred_element_type=F32).astype(BF16)
    slots = slots.reshape(LOCAL, EP, PAD, width)

    vmem = pl.BlockSpec(memory_space=pltpu.VMEM)
    anywhere = pl.BlockSpec(memory_space=pl.ANY)
    hid = pl.pallas_call(
        gather_kernel,
        out_shape=jax.ShapeDtypeStruct((NZ, 2, LOCAL, ROWS, 128), BF16),
        in_specs=[vmem, anywhere, anywhere],
        out_specs=vmem,
        scratch_shapes=[
            pltpu.VMEM((NZ, 2, LOCAL, ROWS, width), BF16),
            pltpu.VMEM((LOCAL, EP, PAD, width), BF16),
            pltpu.VMEM((LOCAL, width, 256), BF16),
            DMA((LOCAL, 2)), DMA((LOCAL, EP)), DMA((LOCAL, EP)),
            DMA((2, STEPS)), DMA((2, STEPS)), DMA((2, STEPS + 1)), DMA((2, STEPS + 1)),
        ],
        cost_estimate=pl.CostEstimate(flops=6 * 10**9, bytes_accessed=3 * 10**8, transcendentals=0),
        compiler_params=pltpu.CompilerParams(
            collective_id=0, has_side_effects=True, vmem_limit_bytes=40 * 2**20
        ),
        name="gather_experts",
    )(slots, w_gate, w_up)
    back = pl.pallas_call(
        scatter_kernel,
        out_shape=jax.ShapeDtypeStruct((LOCAL, EP, PAD, width), BF16),
        in_specs=[vmem, vmem],
        out_specs=vmem,
        scratch_shapes=[
            pltpu.VMEM((2, STEPS + 1, ROWS, width), BF16),
            pltpu.VMEM((2, STEPS + 1, ROWS, width), BF16),
            pltpu.VMEM((2, STEPS, ROWS, width), BF16),
            pltpu.VMEM((2, STEPS, ROWS, width), BF16),
            pltpu.VMEM((LOCAL, EP, PAD, width), BF16),
            DMA((2, STEPS + 1)), DMA((2, STEPS + 1)), DMA((2, STEPS)), DMA((2, STEPS)),
            DMA((LOCAL, EP)), DMA((LOCAL, EP)),
        ],
        cost_estimate=pl.CostEstimate(flops=6 * 10**9, bytes_accessed=3 * 10**8, transcendentals=0),
        compiler_params=pltpu.CompilerParams(
            collective_id=1, has_side_effects=True, vmem_limit_bytes=56 * 2**20
        ),
        name="scatter_experts",
    )(hid, w_down)

    hit = [every[None, :] == slot_ids[:, k : k + 1] for k in range(2)]
    weights = sum(jnp.where(hit[k], route_weights[:, k : k + 1], 0.0) for k in range(2))
    high = lax.reduce_precision(weights, 8, 7)
    low = lax.reduce_precision(weights - high, 8, 7)
    both = jnp.concatenate((high, low), axis=0).astype(BF16)
    sums = jnp.dot(both, back.reshape(wide, width), preferred_element_type=F32)
    expert_out = (sums[:tok_count] + sums[tok_count:]).astype(BF16)

    mixer_out = pl.pallas_call(
        mixer_kernel,
        grid=(NZ * 2,),
        out_shape=jax.ShapeDtypeStruct((tok_count, width), BF16),
        in_specs=[
            pl.BlockSpec((tok_count + 16, width), lambda t: (0, 0)),
            pl.BlockSpec((None, 3, 128), lambda t: (t, 0, 0)),
            pl.BlockSpec((EP, 1, 1, 4, 128, 128), lambda t: (0, t % 2, t // 2, 0, 0, 0)),
        ],
        out_specs=pl.BlockSpec((tok_count, width), lambda t: (0, 0)),
        scratch_shapes=[pltpu.VMEM((tok_count, width), F32)],
        cost_estimate=pl.CostEstimate(flops=5 * 10**9, bytes_accessed=34 * 10**6, transcendentals=0),
        compiler_params=pltpu.CompilerParams(vmem_limit_bytes=24 * 2**20),
        name="mix_tokens",
    )(mix_rows, taps, blocks)
    return (mixer_out, expert_out)


def solution(mesh):
    finer = Mesh(mesh.devices.reshape(mesh.shape["ep"], 8, 2), EP_TP)
    return jax.shard_map(
        per_device,
        mesh=finer,
        in_specs=(
            P(EP_TP, None), P(EP_TP, None), P(), P(None, TP), P(None, TP), P(None, TP),
            P(None, TP), P(TP, None), P(), P("ep", None, TP), P("ep", None, TP),
            P("ep", TP, None), P(EP_TP, None), P(EP_TP, None),
        ),
        out_specs=(P(EP_TP, None), P(EP_TP, None)),
        check_vma=False,
    )
```

```python
import functools

import jax
import jax.numpy as jnp
from jax import lax
from jax.experimental import pallas as pl
from jax.experimental.pallas import tpu as pltpu
from jax.sharding import Mesh
from jax.sharding import PartitionSpec as P

EXPERTS = 32
CAP = 10
QUADS = 80
EIGHTS = 80
EP = 16
NZ = 8
LOCAL = 2
ROWS = EP * CAP
TP = ("tp_0", "tp_1")
EP_TP = ("ep", "tp_0", "tp_1")
MESH = pl.DeviceIdType.MESH
F32 = jnp.float32
BF16 = jnp.bfloat16

norm_eps = 1e-06
clamp_limit = 7.0
gate_alpha = 1.702


def rms_scale(tok_rows, gain_vec):
    values = tok_rows.astype(F32)
    scaled = values * lax.rsqrt(jnp.mean(values * values, axis=-1, keepdims=True) + norm_eps)
    return (scaled * gain_vec).astype(BF16)


def places():
    return lax.axis_index("ep"), lax.axis_index("tp_0"), lax.axis_index("tp_1")


def signal(where):
    pl.semaphore_signal(
        pltpu.get_barrier_semaphore(), inc=1, device_id=where, device_id_type=MESH
    )


def signal_all(count, where):
    def one(k, _):
        signal(where(k))
        return 0

    lax.fori_loop(1, count, one, 0)


def signal_ring(ep, z, core):
    for step in (1, NZ - 1):
        signal((ep, lax.rem(z + step, NZ), core))
    signal((ep, z, 1 - core))


def remote(src, dst, send, recv, where):
    return pltpu.make_async_remote_copy(
        src_ref=src, dst_ref=dst, send_sem=send, recv_sem=recv, device_id=where, device_id_type=MESH
    )


def each(count, act):
    def one(k, _):
        act(k)
        return 0

    lax.fori_loop(1, count, one, 0)


GATHER_D = (1, 1, 2, 2, 3, 3, 4)
GATHER_X = ((0, 1, 0, 1, 0, 1, 0), (0, 1, 0, 1, 0, 1, 1))
SCATTER_D = (4, 3, 3, 2, 2, 1, 1)
SCATTER_X = ((0, 1, 0, 1, 0, 1, 0), (1, 0, 1, 0, 1, 1, 0))
SCATTER_IN = ((None, None, 0, 1, 2, 3, 4), (None, None, 0, 1, 2, 4, 3))
LAST_IN = {1: (5, 5), 0: (6, 6)}
STEPS = 7


def forwards(way, n):
    nxt = 6 if (way, n) == (1, 5) else n + 2
    if nxt < STEPS and GATHER_X[way][nxt] == GATHER_X[way][n] and GATHER_D[nxt] == GATHER_D[n] + 1:
        return nxt
    return None


def exchange_kernel(
    slots, tail, taps, w_outer, w_inner, w_value, w_mix,
    unit, w_three, w_one, taps_all, halo,
    landed, part,
    w_sem, a_send, a_recv, r_send, r_recv, t_send, t_recv, h_sem,
):
    ep, z, core = places()
    own = pl.ds(pl.multiple_of(ep * 128, 128), 128)
    loads = [
        pltpu.make_async_copy(w.at[own], part.at[i], w_sem.at[i])
        for i, w in enumerate((w_inner, w_value, w_outer))
    ]
    loads.append(pltpu.make_async_copy(w_mix.at[:, own], part.at[3], w_sem.at[3]))
    for load in loads:
        load.start()
    spot = z * 2 + core

    def tp_peer(k):
        to = lax.rem(spot + k, NZ * 2)
        return ep, to // 2, lax.rem(to, 2)

    def in_order(step):
        to = lax.rem(ep * (NZ * 2) + spot + step, EP * NZ * 2)
        return to // (NZ * 2), lax.rem(to // 2, NZ), lax.rem(to, 2)

    def ep_peer(k):
        return lax.rem(ep + k, EP), z, core

    signal_all(EP, ep_peer)
    signal_all(NZ * 2, tp_peer)
    signal(in_order(1))
    signal(in_order(EP * NZ * 2 - 1))
    pl.semaphore_wait(pltpu.get_barrier_semaphore(), EP + NZ * 2)

    def exchange(k):
        where = ep_peer(k)
        return remote(slots.at[where[0]], landed.at[ep], a_send.at[k], a_recv.at[k], where)

    def tell_taps(k):
        return remote(taps, taps_all.at[spot], t_send.at[k], t_recv.at[k], tp_peer(k))

    def tell_tail():
        return remote(tail, halo, h_sem.at[0], h_sem.at[1], in_order(1))

    steps = (NZ - 1, 1)

    def ring_copies(way, n):
        away = GATHER_D[n] - 1
        at = lax.rem(z + away * steps[way], NZ)
        there = (ep, lax.rem(z + (NZ - steps[way]), NZ), core)
        if GATHER_X[way][n] == 0:
            pairs = [(part.at[0:2] if away == 0 else w_three.at[at, 0:2], w_three.at[at, 0:2])]
        else:
            pairs = [
                (part.at[2] if away == 0 else w_three.at[at, 2], w_three.at[at, 2]),
                (part.at[3] if away == 0 else w_one.at[at], w_one.at[at]),
            ]
        return [
            remote(src, dst, r_send.at[way, n, i], r_recv.at[way, n, i], there)
            for i, (src, dst) in enumerate(pairs)
        ]

    for load in loads:
        load.wait()
    for n in range(LOCAL):
        for way in range(2):
            for copy in ring_copies(way, n):
                copy.start()
    each(EP, lambda k: exchange(k).start())
    each(NZ * 2, lambda k: tell_taps(k).start())
    tell_tail().start()
    w_three[z] = part[0:3]
    w_one[z] = part[3]
    taps_all[spot] = taps[...]
    landed[ep] = slots[ep]
    row = lax.broadcasted_iota(jnp.int32, (LOCAL * ROWS, EP * QUADS), 0)
    col = lax.broadcasted_iota(jnp.int32, (LOCAL * ROWS, EP * QUADS), 1)
    x, src, slot = row // ROWS, (row % ROWS) // CAP, row % CAP
    first = src * QUADS + x * CAP + slot
    for n in range(STEPS):
        for way in range(2):
            for copy in ring_copies(way, n):
                copy.wait_recv()
            nxt = forwards(way, n)
            if nxt is not None:
                for copy in ring_copies(way, nxt):
                    copy.start()
    each(EP, lambda k: exchange(k).wait_recv())
    for block in range(4):
        picks = (first + block * (LOCAL * CAP) == col).astype(BF16)
        out = jnp.dot(picks, landed[...].reshape(EP * QUADS, 512), preferred_element_type=F32)
        unit[:, :, block * 512 : (block + 1) * 512] = out.astype(BF16).reshape(LOCAL, ROWS, 512)
    each(NZ * 2, lambda k: tell_taps(k).wait())
    tell_tail().wait()
    each(EP, lambda k: exchange(k).wait_send())
    for way in range(2):
        for n in range(STEPS):
            for copy in ring_copies(way, n):
                copy.wait_send()


def gather_kernel(
    unit, w_gate, w_up, hid,
    units, w_both,
    w_sem, r_send, r_recv, c_send, c_recv,
):
    ep, z, core = places()
    loads = []
    for x in range(LOCAL):
        loads.append(pltpu.make_async_copy(w_gate.at[x], w_both.at[x, :, 0:128], w_sem.at[x, 0]))
        loads.append(pltpu.make_async_copy(w_up.at[x], w_both.at[x, :, 128:256], w_sem.at[x, 1]))
    for load in loads:
        load.start()
    signal_ring(ep, z, core)
    pl.semaphore_wait(pltpu.get_barrier_semaphore(), 3)

    def compute(tok, at_z, at_core, x):
        both = jnp.dot(tok, w_both[x], preferred_element_type=F32)
        gate_pre = jnp.minimum(both[:, 0:128], clamp_limit)
        up_pre = jnp.clip(both[:, 128:256], -clamp_limit, clamp_limit)
        hid[at_z, at_core, x] = (
            (up_pre + 1.0) * gate_pre * jax.nn.sigmoid(gate_alpha * gate_pre)
        ).astype(BF16)

    steps = (NZ - 1, 1)

    def ring_copy(way, n):
        away = GATHER_D[n] - 1
        at = lax.rem(z + away * steps[way], NZ)
        x = GATHER_X[way][n]
        there = lax.rem(z + (NZ - steps[way]), NZ)
        return remote(
            unit.at[x] if away == 0 else units.at[at, core, x], units.at[at, core, x],
            r_send.at[way, n], r_recv.at[way, n], (ep, there, core),
        )

    def across(way, n):
        own = n == STEPS
        at = z if own else lax.rem(z + GATHER_D[n] * steps[way], NZ)
        x = way if own else GATHER_X[way][n]
        ref = units.at[at, core, x]
        copy = remote(
            unit.at[x] if own else ref, ref, c_send.at[way, n], c_recv.at[way, n], (ep, z, 1 - core)
        )
        return copy, at, x

    for n in range(LOCAL):
        for way in range(2):
            ring_copy(way, n).start()
    for way in range(2):
        across(way, STEPS)[0].start()
    for load in loads:
        load.wait()
    for x in range(LOCAL):
        compute(unit[x], z, core, x)

    for n in range(STEPS):
        for way in range(2):
            ring_copy(way, n).wait_recv()
            nxt = forwards(way, n)
            if nxt is not None:
                ring_copy(way, nxt).start()
            across(way, n)[0].start()
        for way in range(2):
            at = lax.rem(z + GATHER_D[n] * steps[way], NZ)
            x = GATHER_X[way][n]
            compute(units[at, core, x], at, core, x)
        for way in range(2):
            copy, at, x = across(way, STEPS if n == 0 else n - 1)
            copy.wait_recv()
            compute(units[at, 1 - core, x], at, 1 - core, x)
    for way in range(2):
        copy, at, x = across(way, STEPS - 1)
        copy.wait_recv()
        compute(units[at, 1 - core, x], at, 1 - core, x)
    for way in range(2):
        for n in range(STEPS):
            ring_copy(way, n).wait_send()
            across(way, n)[0].wait_send()
        across(way, STEPS)[0].wait_send()


def scatter_kernel(
    hid, w_down, tok, taps, w_three,
    back, gated,
    c_out, c_in, r_out, r_in, b_in, b_out, spread, w_slots,
    c_send, c_recv, r_send, r_recv, a_send, a_recv, w_sem,
):
    ep, z, core = places()

    def fetch(t):
        return pltpu.make_async_copy(
            w_three.at[:, lax.rem(t, 2), t // 2], w_slots.at[lax.rem(t, 2)], w_sem.at[lax.rem(t, 2)]
        )

    fetch(0).start()
    fetch(1).start()
    signal_all(EP, lambda k: (lax.rem(ep + k, EP), z, core))
    signal_ring(ep, z, core)
    pl.semaphore_wait(pltpu.get_barrier_semaphore(), EP + 2)

    def mix(t, _):
        fetch(t).wait()
        at = lax.rem(t, 2)
        rows = tok[...]
        pair = jnp.concatenate([w_slots[at, :, i].reshape(2048, 128) for i in range(2)], axis=1)
        pair = jnp.dot(rows, pair, preferred_element_type=F32)
        prod = pair[:, 0:128] * pair[:, 128:256]
        outer = jnp.dot(
            rows[16:144], w_slots[at, :, 2].reshape(2048, 128), preferred_element_type=F32
        )
        tap = taps[t]
        conv = tap[2:3] * prod[16:144] + tap[1:2] * prod[15:143] + tap[0:1] * prod[14:142]
        gated[lax.rem(t, 2), t // 2] = (outer * conv).astype(BF16)

        @pl.when(t + 2 < NZ * 2)
        def _():
            fetch(t + 2).start()

        return 0
    steps = (1, NZ - 1)

    def place(way, m):
        if m == STEPS:
            return z, way
        return lax.rem(z + SCATTER_D[m] * steps[way], NZ), SCATTER_X[way][m]

    def across(way, m):
        return remote(
            c_out.at[way, m], c_in.at[way, m], c_send.at[way, m], c_recv.at[way, m],
            (ep, z, 1 - core),
        )

    def ring_copy(way, m):
        return remote(
            r_out.at[way, m], r_in.at[way, m], r_send.at[way, m], r_recv.at[way, m],
            (ep, lax.rem(z + steps[way], NZ), core),
        )

    def partial(at, at_core, x, add, out):
        def tile(j, _):
            cols = pl.ds(pl.multiple_of(j * 512, 512), 512)
            total = jnp.dot(hid[at, at_core, x], w_down[x, :, cols], preferred_element_type=F32)
            for ref in add:
                total = total + ref[:, cols].astype(F32)
            out[:, cols] = total.astype(BF16)
            return 0

        lax.fori_loop(0, 4, tile, 0)

    def help_other(m):
        for way in range(2):
            at, x = place(way, m)
            partial(at, 1 - core, x, (), c_out.at[way, m])
            across(way, m).start()

    help_other(0)
    help_other(1)
    for m in range(STEPS):
        for way in range(2):
            at, x = place(way, m)
            add = [c_in.at[way, m]]
            across(way, m).wait_recv()
            came = SCATTER_IN[way][m]
            if came is not None:
                ring_copy(way, came).wait_recv()
                add.append(r_in.at[way, came])
            partial(at, core, x, add, r_out.at[way, m])
            ring_copy(way, m).start()
        if m + 2 <= STEPS:
            help_other(m + 2)
        if m == 1:
            row = lax.broadcasted_iota(jnp.int32, spread.shape, 0)
            col = lax.broadcasted_iota(jnp.int32, spread.shape, 1)
            want = ((row % EIGHTS) // CAP) * ROWS + (row // EIGHTS) * CAP + row % CAP
            spread[...] = (want == col).astype(BF16)
        if m > 1:
            lax.fori_loop((m - 2) * 4, min((m - 1) * 4, NZ * 2), mix, 0)

    def exchange(x, k):
        to = lax.rem(ep + k, EP)
        return remote(
            b_out.at[x, to], back.at[x, ep], a_send.at[x, k], a_recv.at[x, k], (to, z, core)
        )

    for x in (1, 0):
        across(x, STEPS).wait_recv()
        for way in range(2):
            ring_copy(way, LAST_IN[x][way]).wait_recv()

        def tile(j, _, x=x):
            cols = pl.ds(pl.multiple_of(j * 256, 256), 256)
            total = jnp.dot(hid[z, core, x], w_down[x, :, cols], preferred_element_type=F32)
            for ref in (c_in.at[x, STEPS], r_in.at[0, LAST_IN[x][0]], r_in.at[1, LAST_IN[x][1]]):
                total = total + ref[:, cols].astype(F32)
            b_in[j] = total.astype(BF16)
            return 0

        lax.fori_loop(0, 8, tile, 0)

        def spread_out(j, _, x=x):
            rows = pl.ds(pl.multiple_of(j * (4 * EIGHTS), 4 * EIGHTS), 4 * EIGHTS)
            wide = jnp.dot(spread[rows, :], b_in[...].reshape(8 * ROWS, 256), preferred_element_type=F32)
            b_out[x, pl.ds(j * 4, 4)] = wide.astype(BF16).reshape(4, EIGHTS, 256)
            return 0

        lax.fori_loop(0, 4, spread_out, 0)

        def send_one(k, _, x=x):
            exchange(x, k).start()
            return 0

        lax.fori_loop(1, EP, send_one, 0)
        back[x, ep] = b_out[x, ep]
    for way in range(2):
        for m in range(STEPS):
            ring_copy(way, m).wait_send()
            across(way, m).wait_send()
        across(way, STEPS).wait_send()
    for x in (1, 0):

        def end_one(k, _, x=x):
            exchange(x, k).wait()
            return 0

        lax.fori_loop(1, EP, end_one, 0)


def last_product_kernel(gated, w_one, out):
    rows = jnp.concatenate([gated[i, j] for i in range(2) for j in range(NZ)], axis=1)
    pair = jnp.concatenate([w_one[i].reshape(2048, 128) for i in range(2)], axis=1)
    out[...] = jnp.dot(rows, pair, preferred_element_type=F32).astype(BF16)


def slot_places(route_ids):
    flat_ids = route_ids.reshape(-1)
    member = (flat_ids[:, None] == jnp.arange(EXPERTS, dtype=jnp.int32)[None, :]).astype(jnp.int32)
    earlier = jnp.cumsum(member, axis=0) - member
    place = jnp.sum(earlier * member, axis=1)
    shape = route_ids.shape
    return (flat_ids // LOCAL).reshape(shape), (flat_ids % LOCAL).reshape(shape), place.reshape(shape)


DMA = pltpu.SemaphoreType.DMA


def per_device(
    mixer_in, expert_in, mixer_gain, w_outer, w_inner, w_value, conv_taps, w_mix_out,
    expert_gain, w_gate, w_up, w_down, route_ids, route_weights,
):
    tok_count, width = expert_in.shape
    normed_mix = rms_scale(mixer_in, mixer_gain)
    normed_exp = rms_scale(expert_in, expert_gain)
    owner, which, place = slot_places(route_ids)

    out_row = owner * QUADS + which * CAP + place
    rows_out = jnp.arange(EP * QUADS, dtype=jnp.int32)[:, None]
    placing = jnp.concatenate(
        [
            (
                (rows_out == out_row[None, :, 0] + q * (LOCAL * CAP))
                | (rows_out == out_row[None, :, 1] + q * (LOCAL * CAP))
            ).astype(BF16)
            for q in range(4)
        ],
        axis=1,
    )
    stacked = jnp.concatenate([normed_exp[:, q * 512 : (q + 1) * 512] for q in range(4)], axis=0)
    slots = jnp.dot(placing, stacked, preferred_element_type=F32).astype(BF16)
    slots = slots.reshape(EP, QUADS, 512)
    taps = jnp.concatenate((conv_taps, jnp.zeros((5, 128), F32)), axis=0)

    vmem = pl.BlockSpec(memory_space=pltpu.VMEM)
    anywhere = pl.BlockSpec(memory_space=pl.ANY)
    unit, w_three, w_one, taps_all, halo = pl.pallas_call(
        exchange_kernel,
        out_shape=(
            jax.ShapeDtypeStruct((LOCAL, ROWS, width), BF16),
            jax.ShapeDtypeStruct((NZ, 3, 128, 128), BF16),
            jax.ShapeDtypeStruct((NZ, 128, 128), BF16),
            jax.ShapeDtypeStruct((NZ * 2, 8, 128), F32),
            jax.ShapeDtypeStruct((16, width), BF16),
        ),
        in_specs=[vmem] * 3 + [anywhere] * 4,
        out_specs=(vmem,) * 5,
        scratch_shapes=[
            pltpu.VMEM((EP, QUADS, 512), BF16),
            pltpu.VMEM((4, 128, 128), BF16),
            DMA((4,)), DMA((EP,)), DMA((EP,)), DMA((2, STEPS, 2)), DMA((2, STEPS, 2)),
            DMA((NZ * 2,)), DMA((NZ * 2,)), DMA((2,)),
        ],
        cost_estimate=pl.CostEstimate(flops=2 * 10**10, bytes_accessed=10**7, transcendentals=0),
        compiler_params=pltpu.CompilerParams(
            collective_id=0, has_side_effects=True, vmem_limit_bytes=24 * 2**20
        ),
        name="exchange",
    )(slots, normed_mix[tok_count - 16 :], taps, w_outer, w_inner, w_value, w_mix_out)

    w_three = lax.all_gather(w_three, ("ep", "tp_1"), axis=0, tiled=False)
    w_one = lax.all_gather(w_one, ("ep", "tp_1"), axis=0, tiled=False)
    w_three = w_three.reshape(EP, 2, NZ, 3, 128, 128)
    w_one = w_one.reshape(EP, 2, NZ, 128, 128)

    hid = pl.pallas_call(
        gather_kernel,
        out_shape=jax.ShapeDtypeStruct((NZ, 2, LOCAL, ROWS, 128), BF16),
        in_specs=[vmem, anywhere, anywhere],
        out_specs=vmem,
        scratch_shapes=[
            pltpu.VMEM((NZ, 2, LOCAL, ROWS, width), BF16),
            pltpu.VMEM((LOCAL, width, 256), BF16),
            DMA((LOCAL, 2)),
            DMA((2, STEPS)), DMA((2, STEPS)), DMA((2, STEPS + 1)), DMA((2, STEPS + 1)),
        ],
        cost_estimate=pl.CostEstimate(flops=10**11, bytes_accessed=3 * 10**8, transcendentals=0),
        compiler_params=pltpu.CompilerParams(
            collective_id=1, has_side_effects=True, vmem_limit_bytes=40 * 2**20
        ),
        name="gather_experts",
    )(unit, w_gate, w_up)

    ep, z, core = places()
    halo = jnp.where((ep == 0) & (z == 0) & (core == 0), jnp.zeros_like(halo), halo)
    mix_rows = jnp.concatenate((halo, normed_mix), axis=0)
    back, gated = pl.pallas_call(
        scatter_kernel,
        out_shape=(
            jax.ShapeDtypeStruct((LOCAL, EP, EIGHTS, 256), BF16),
            jax.ShapeDtypeStruct((2, NZ, tok_count, 128), BF16),
        ),
        in_specs=[vmem] * 4 + [anywhere],
        out_specs=(vmem, vmem),
        scratch_shapes=[
            pltpu.VMEM((2, STEPS + 1, ROWS, width), BF16),
            pltpu.VMEM((2, STEPS + 1, ROWS, width), BF16),
            pltpu.VMEM((2, STEPS, ROWS, width), BF16),
            pltpu.VMEM((2, STEPS, ROWS, width), BF16),
            pltpu.VMEM((8, ROWS, 256), BF16),
            pltpu.VMEM((LOCAL, EP, EIGHTS, 256), BF16),
            pltpu.VMEM((EP * EIGHTS, 8 * ROWS), BF16),
            pltpu.VMEM((2, EP, 3, 128, 128), BF16),
            DMA((2, STEPS + 1)), DMA((2, STEPS + 1)), DMA((2, STEPS)), DMA((2, STEPS)),
            DMA((LOCAL, EP)), DMA((LOCAL, EP)), DMA((2,)),
        ],
        cost_estimate=pl.CostEstimate(flops=10**11, bytes_accessed=3 * 10**8, transcendentals=0),
        compiler_params=pltpu.CompilerParams(
            collective_id=2, has_side_effects=True, vmem_limit_bytes=58 * 2**20
        ),
        name="scatter_experts",
    )(hid, w_down, mix_rows, taps_all, w_three)

    back_row = which * (EP * EIGHTS) + owner * EIGHTS + place
    rows_back = jnp.arange(LOCAL * EP * EIGHTS, dtype=jnp.int32)[None, :]
    back = back.reshape(LOCAL * EP * EIGHTS, 256)
    blocks = []
    for q in range(8):
        weights = sum(
            jnp.where(
                rows_back == back_row[:, k : k + 1] + q * CAP, route_weights[:, k : k + 1], 0.0
            )
            for k in range(2)
        )
        high = lax.reduce_precision(weights, 8, 7)
        low = lax.reduce_precision(weights - high, 8, 7)
        both = jnp.concatenate((high, low), axis=0).astype(BF16)
        sums = jnp.dot(both, back, preferred_element_type=F32)
        blocks.append((sums[:tok_count] + sums[tok_count:]).astype(BF16))
    expert_out = jnp.concatenate(blocks, axis=1)

    mixer_out = pl.pallas_call(
        last_product_kernel,
        grid=(EP // 2,),
        out_shape=jax.ShapeDtypeStruct((tok_count, width), BF16),
        in_specs=[
            pl.BlockSpec((2, NZ, tok_count, 128), lambda e: (0, 0, 0, 0)),
            pl.BlockSpec((2, 2, NZ, 128, 128), lambda e: (e, 0, 0, 0, 0)),
        ],
        out_specs=pl.BlockSpec((tok_count, 256), lambda e: (0, e)),
        cost_estimate=pl.CostEstimate(flops=10**9, bytes_accessed=9 * 10**6, transcendentals=0),
        compiler_params=pltpu.CompilerParams(vmem_limit_bytes=16 * 2**20),
        name="last_product",
    )(gated, w_one)
    return (mixer_out, expert_out)


def solution(mesh):
    finer = Mesh(mesh.devices.reshape(mesh.shape["ep"], 8, 2), EP_TP)
    return jax.shard_map(
        per_device,
        mesh=finer,
        in_specs=(
            P(EP_TP, None), P(EP_TP, None), P(), P(None, TP), P(None, TP), P(None, TP),
            P(None, TP), P(TP, None), P(), P("ep", None, TP), P("ep", None, TP),
            P("ep", TP, None), P(EP_TP, None), P(EP_TP, None),
        ),
        out_specs=(P(EP_TP, None), P(EP_TP, None)),
        check_vma=False,
    )
```

```python
import functools

import jax
import jax.numpy as jnp
from jax import lax
from jax.experimental import pallas as pl
from jax.experimental.pallas import tpu as pltpu
from jax.sharding import Mesh
from jax.sharding import PartitionSpec as P

EXPERTS = 32
CAP = 10
QUADS = 80
EIGHTS = 80
EP = 16
NZ = 8
LOCAL = 2
ROWS = EP * CAP
TP = ("tp_0", "tp_1")
EP_TP = ("ep", "tp_0", "tp_1")
MESH = pl.DeviceIdType.MESH
F32 = jnp.float32
BF16 = jnp.bfloat16

norm_eps = 1e-06
clamp_limit = 7.0
gate_alpha = 1.702


def normed(values, gain):
    scaled = values * lax.rsqrt(jnp.mean(values * values, axis=-1, keepdims=True) + norm_eps)
    return (scaled * gain).astype(BF16)


def places():
    return lax.axis_index("ep"), lax.axis_index("tp_0"), lax.axis_index("tp_1")


def signal(where):
    pl.semaphore_signal(
        pltpu.get_barrier_semaphore(), inc=1, device_id=where, device_id_type=MESH
    )


def signal_all(count, where):
    def one(k, _):
        signal(where(k))
        return 0

    lax.fori_loop(1, count, one, 0)


def signal_ring(ep, z, core):
    for step in (1, NZ - 1):
        signal((ep, lax.rem(z + step, NZ), core))
    signal((ep, z, 1 - core))


def remote(src, dst, send, recv, where):
    return pltpu.make_async_remote_copy(
        src_ref=src, dst_ref=dst, send_sem=send, recv_sem=recv, device_id=where, device_id_type=MESH
    )


def each(count, act):
    def one(k, _):
        act(k)
        return 0

    lax.fori_loop(1, count, one, 0)


GATHER_D = (1, 1, 2, 2, 3, 3, 4)
GATHER_X = ((0, 1, 0, 1, 0, 1, 0), (0, 1, 0, 1, 0, 1, 1))
SCATTER_D = (4, 3, 3, 2, 2, 1, 1)
SCATTER_X = ((0, 1, 0, 1, 0, 1, 0), (1, 0, 1, 0, 1, 1, 0))
SCATTER_IN = ((None, None, 0, 1, 2, 3, 4), (None, None, 0, 1, 2, 4, 3))
LAST_IN = {1: (5, 5), 0: (6, 6)}
STEPS = 7


def forwards(way, n):
    nxt = 6 if (way, n) == (1, 5) else n + 2
    if nxt < STEPS and GATHER_X[way][nxt] == GATHER_X[way][n] and GATHER_D[nxt] == GATHER_D[n] + 1:
        return nxt
    return None


LINE = (0, 3, 1, 2)
KINDS = 10


def gather_kernel(
    mixer_in, expert_in, mixer_gain, expert_gain, ids, taps, w_outer, w_inner, w_value, w_mix, w_gate, w_up,
    hid, mix_rows, taps_all, wall,
    stacked, slots, landed, part, wz, tail, halo, unit, units, w_both,
    w_sem, g_sem, a_send, a_recv, z_send, z_recv, t_send, t_recv, h_sem,
    r_send, r_recv, c_send, c_recv, x_send, x_recv, d_send, d_recv, o_sem,
):
    ep, z, core = places()
    own = pl.ds(pl.multiple_of(ep * 128, 128), 128)
    loads = [
        pltpu.make_async_copy(w.at[own], part.at[i], w_sem.at[i])
        for i, w in enumerate((w_inner, w_value, w_outer))
    ]
    loads.append(pltpu.make_async_copy(w_mix.at[:, own], part.at[3], w_sem.at[3]))
    for load in loads:
        load.start()
    gate_loads = []
    for x in range(LOCAL):
        gate_loads.append(pltpu.make_async_copy(w_gate.at[x], w_both.at[x, :, 0:128], g_sem.at[x, 0]))
        gate_loads.append(pltpu.make_async_copy(w_up.at[x], w_both.at[x, :, 128:256], g_sem.at[x, 1]))
    for load in gate_loads:
        load.start()
    spot = z * 2 + core
    partner = (ep, z, 1 - core)

    def tp_peer(k):
        to = lax.rem(spot + k, NZ * 2)
        return ep, to // 2, lax.rem(to, 2)

    def in_order(step):
        to = lax.rem(ep * (NZ * 2) + spot + step, EP * NZ * 2)
        return to // (NZ * 2), lax.rem(to // 2, NZ), lax.rem(to, 2)

    def ep_peer(k):
        return lax.rem(ep + k, EP), z, core

    signal_all(EP, ep_peer)
    signal_all(NZ * 2, tp_peer)
    signal(in_order(1))
    signal(in_order(EP * NZ * 2 - 1))

    def exchange(k):
        where = ep_peer(k)
        return remote(slots.at[where[0]], landed.at[ep], a_send.at[k], a_recv.at[k], where)

    def tell_taps(k):
        return remote(taps, taps_all.at[spot], t_send.at[k], t_recv.at[k], tp_peer(k))

    def tell_tail():
        return remote(tail, halo, h_sem.at[0], h_sem.at[1], in_order(1))

    steps = (NZ - 1, 1)

    def spread_z(way, n):
        away = GATHER_D[n] - 1
        at = lax.rem(z + away * steps[way], NZ)
        there = (ep, lax.rem(z + (NZ - steps[way]), NZ), core)
        two = pl.ds(2 * GATHER_X[way][n], 2)
        return remote(
            part.at[two] if away == 0 else wz.at[at, two], wz.at[at, two],
            z_send.at[way, n], z_recv.at[way, n], there,
        )

    def ring_copy(way, n):
        away = GATHER_D[n] - 1
        at = lax.rem(z + away * steps[way], NZ)
        x = GATHER_X[way][n]
        there = lax.rem(z + (NZ - steps[way]), NZ)
        return remote(
            unit.at[x] if away == 0 else units.at[at, core, x], units.at[at, core, x],
            r_send.at[way, n], r_recv.at[way, n], (ep, there, core),
        )

    def across(way, n):
        mine = n == STEPS
        at = z if mine else lax.rem(z + GATHER_D[n] * steps[way], NZ)
        x = way if mine else GATHER_X[way][n]
        ref = units.at[at, core, x]
        copy = remote(unit.at[x] if mine else ref, ref, c_send.at[way, n], c_recv.at[way, n], partner)
        return copy, at, x

    at_x, at_y = lax.rem(ep, 4), ep // 4

    def off(half, du, dv):
        dx, dy = (du, dv) if half == 0 else (dv, du)
        return lax.rem(at_y + dy, 4) * 4 + lax.rem(at_x + dx, 4)

    def piece(half, way, kind, e, at_core):
        whole = kind == 0 or 2 <= kind < 6
        zs = pl.ds(4 * half, 4) if whole else pl.ds(4 * half + 2 * way, 2)
        return wall.at[e, at_core, zs]

    def plane(half, way, kind):
        step = 1 if way == 0 else 3
        if kind == 0:
            e, to = ep, off(half, step, 0)
        elif kind == 1:
            e, to = off(half, 4 - step, 0), off(half, step, 0)
        elif kind < 6:
            e, to = off(half, LINE[kind - 2], 0), off(half, 0, step)
        else:
            e, to = off(half, LINE[kind - 6], 4 - step), off(half, 0, step)
        ref = piece(half, way, kind, e, core)
        return remote(
            wz.at[pl.ds(4 * half, 4)] if kind in (0, 2) else ref, ref,
            x_send.at[half, way, kind], x_recv.at[half, way, kind], (to, z, core),
        )

    def plane_over(half, way, kind):
        step = 1 if way == 0 else 3
        if kind == 0:
            e = off(half, 4 - step, 0)
        elif kind == 1:
            e = off(half, 2, 0)
        elif kind < 6:
            e = off(half, LINE[kind - 2], 4 - step)
        else:
            e = off(half, LINE[kind - 6], 2)
        ref = piece(half, way, kind, e, core)
        return remote(ref, ref, d_send.at[half, way, kind], d_recv.at[half, way, kind], partner)

    both_halves = [(half, way) for half in range(2) for way in range(2)]

    def take(*kinds):
        for kind in kinds:
            for half, way in both_halves:
                plane(half, way, kind).wait_recv()
                plane_over(half, way, kind).start()

    def give(*kinds):
        for kind in kinds:
            for half, way in both_halves:
                plane(half, way, kind).start()

    def own_over():
        ref = wall.at[ep, core]
        return remote(wz, ref, o_sem.at[0], o_sem.at[1], partner)

    def own_keep():
        return pltpu.make_async_copy(wz, wall.at[ep, core], o_sem.at[2])

    def compute(tok, at_z, at_core, x):
        both = jnp.dot(tok, w_both[x], preferred_element_type=F32)
        gate_pre = jnp.minimum(both[:, 0:128], clamp_limit)
        up_pre = jnp.clip(both[:, 128:256], -clamp_limit, clamp_limit)
        hid[at_z, at_core, x] = (
            (up_pre + 1.0) * gate_pre * jax.nn.sigmoid(gate_alpha * gate_pre)
        ).astype(BF16)

    def pass_z(n):
        for way in range(2):
            spread_z(way, n).wait_recv()
            nxt = forwards(way, n)
            if nxt is not None:
                spread_z(way, nxt).start()

    pl.semaphore_wait(pltpu.get_barrier_semaphore(), EP + NZ * 2)
    for load in loads:
        load.wait()
    for n in range(LOCAL):
        for way in range(2):
            spread_z(way, n).start()
    each(NZ * 2, lambda k: tell_taps(k).start())
    rows = normed(expert_in[...].astype(F32), expert_gain[...])
    for q in range(4):
        stacked[q * 128 : (q + 1) * 128] = rows[:, q * 512 : (q + 1) * 512]

    experts = lax.broadcasted_iota(jnp.int32, (EXPERTS, 128), 0)
    hits = [experts == ids[k : k + 1, :] for k in range(2)]
    member = (hits[0] | hits[1]).astype(BF16)
    before = lax.broadcasted_iota(jnp.int32, (128, 128), 0) < lax.broadcasted_iota(jnp.int32, (128, 128), 1)
    earlier = jnp.dot(member, before.astype(BF16), preferred_element_type=F32)
    goes = []
    for k in range(2):
        place = jnp.sum(jnp.where(hits[k], earlier, 0.0), axis=0, keepdims=True).astype(jnp.int32)
        one = ids[k : k + 1, :]
        goes.append((one >> 1) * QUADS + (one & 1) * CAP + place)

    def fill(j, _):
        row = lax.broadcasted_iota(jnp.int32, (4 * QUADS, 128), 0) + j * (4 * QUADS)
        placing = jnp.concatenate(
            [
                ((row == goes[0] + q * (LOCAL * CAP)) | (row == goes[1] + q * (LOCAL * CAP))).astype(F32)
                for q in range(4)
            ],
            axis=1,
        ).astype(BF16)
        out = jnp.dot(placing, stacked[...], preferred_element_type=F32)
        slots[pl.ds(j * 4, 4)] = out.astype(BF16).reshape(4, QUADS, 512)
        return 0

    lax.fori_loop(0, 4, fill, 0)
    each(EP, lambda k: exchange(k).start())
    landed[ep] = slots[ep]
    pass_z(0)
    rows = normed(mixer_in[...].astype(F32), mixer_gain[...])
    mix_rows[16:144] = rows
    tail[...] = rows[112:128]
    tell_tail().start()
    wz[z] = part[...]
    taps_all[spot] = taps[...]
    for n in range(1, STEPS):
        pass_z(n)
    give(0)
    give(2)
    own_over().start()
    own_keep().start()
    row = lax.broadcasted_iota(jnp.int32, (LOCAL * ROWS, EP * QUADS), 0)
    col = lax.broadcasted_iota(jnp.int32, (LOCAL * ROWS, EP * QUADS), 1)
    x, src, slot = row // ROWS, (row % ROWS) // CAP, row % CAP
    first = src * QUADS + x * CAP + slot
    each(EP, lambda k: exchange(k).wait_recv())
    for block in range(4):
        picks = (first + block * (LOCAL * CAP) == col).astype(BF16)
        out = jnp.dot(picks, landed[...].reshape(EP * QUADS, 512), preferred_element_type=F32)
        unit[:, :, block * 512 : (block + 1) * 512] = out.astype(BF16).reshape(LOCAL, ROWS, 512)
    for n in range(LOCAL):
        for way in range(2):
            ring_copy(way, n).start()
    for way in range(2):
        across(way, STEPS)[0].start()
    tell_tail().wait()
    lone = (ep == 0) & (spot == 0)
    mix_rows[0:16] = jnp.where(lone, jnp.zeros_like(halo), halo[...])
    each(NZ * 2, lambda k: tell_taps(k).wait())
    for load in gate_loads:
        load.wait()
    for x in range(LOCAL):
        compute(unit[x], z, core, x)

    for n in range(STEPS):
        for way in range(2):
            ring_copy(way, n).wait_recv()
            nxt = forwards(way, n)
            if nxt is not None:
                ring_copy(way, nxt).start()
            across(way, n)[0].start()
        if n == 0:
            take(0)
            give(1, 3, 4)
        elif n == 1:
            take(2)
            give(6)
        elif n == 2:
            take(1)
            give(5)
        elif n == 3:
            take(3, 4)
            give(7, 8)
        elif n == 4:
            take(6)
        elif n == 5:
            take(5)
            give(9)
            take(7, 8)
        for way in range(2):
            at = lax.rem(z + GATHER_D[n] * steps[way], NZ)
            x = GATHER_X[way][n]
            compute(units[at, core, x], at, core, x)
        for way in range(2):
            copy, at, x = across(way, STEPS if n == 0 else n - 1)
            copy.wait_recv()
            compute(units[at, 1 - core, x], at, 1 - core, x)
    for way in range(2):
        copy, at, x = across(way, STEPS - 1)
        copy.wait_recv()
        compute(units[at, 1 - core, x], at, 1 - core, x)
    take(9)
    own_keep().wait()
    own_over().wait()
    for half, way in both_halves:
        for kind in range(KINDS):
            plane(half, way, kind).wait_send()
            plane_over(half, way, kind).wait()
    each(EP, lambda k: exchange(k).wait_send())
    for way in range(2):
        for n in range(STEPS):
            spread_z(way, n).wait_send()
            ring_copy(way, n).wait_send()
            across(way, n)[0].wait_send()
        across(way, STEPS)[0].wait_send()


def scatter_kernel(
    hid, w_down, tok, taps, ids, weights, wall,
    mixer_out, expert_out,
    c_out, c_in, r_out, r_in, b_in, b_out, back, spread, gather, shares, sums, gated, w_slots, l_slots,
    c_send, c_recv, r_send, r_recv, a_send, a_recv, w_sem, l_sem,
):
    ep, z, core = places()

    def fetch(t):
        return pltpu.make_async_copy(
            wall.at[:, lax.rem(t, 2), t // 2, 0:3], w_slots.at[lax.rem(t, 2)], w_sem.at[lax.rem(t, 2)]
        )

    def fetch_last(j):
        return pltpu.make_async_copy(
            wall.at[pl.ds(2 * j, 2), :, :, 3], l_slots.at[lax.rem(j, 2)], l_sem.at[lax.rem(j, 2)]
        )

    for t in range(2):
        fetch(t).start()
        fetch_last(t).start()
    signal_all(EP, lambda k: (lax.rem(ep + k, EP), z, core))
    signal_ring(ep, z, core)
    pl.semaphore_wait(pltpu.get_barrier_semaphore(), EP + 2)

    def mix(t, _):
        fetch(t).wait()
        at = lax.rem(t, 2)
        rows = tok[...]
        pair = jnp.concatenate([w_slots[at, :, i].reshape(2048, 128) for i in range(2)], axis=1)
        pair = jnp.dot(rows, pair, preferred_element_type=F32)
        prod = pair[:, 0:128] * pair[:, 128:256]
        outer = jnp.dot(
            rows[16:144], w_slots[at, :, 2].reshape(2048, 128), preferred_element_type=F32
        )
        tap = taps[t]
        conv = tap[2:3] * prod[16:144] + tap[1:2] * prod[15:143] + tap[0:1] * prod[14:142]
        gated[t] = (outer * conv).astype(BF16)

        @pl.when(t + 2 < NZ * 2)
        def _():
            fetch(t + 2).start()

        return 0

    def last(j, _):
        fetch_last(j).wait()
        at = lax.rem(j, 2)
        rows = jnp.concatenate([gated[i * 2 + c] for c in range(2) for i in range(NZ)], axis=1)
        pair = jnp.concatenate([l_slots[at, i].reshape(2048, 128) for i in range(2)], axis=1)
        cols = pl.ds(pl.multiple_of(j * 256, 256), 256)
        mixer_out[:, cols] = jnp.dot(rows, pair, preferred_element_type=F32).astype(BF16)

        @pl.when(j + 2 < EP // 2)
        def _():
            fetch_last(j + 2).start()

        return 0

    def tables():
        def fill(j, _):
            rows = pl.ds(pl.multiple_of(j * 320, 320), 320)
            row = lax.broadcasted_iota(jnp.int32, (320, spread.shape[1]), 0) + j * 320
            col = lax.broadcasted_iota(jnp.int32, (320, spread.shape[1]), 1)
            slot = lax.rem(row, CAP)
            to = lax.rem(row, EIGHTS) // CAP * ROWS + row // EIGHTS * CAP + slot
            spread[rows] = (to == col).astype(BF16)
            to = lax.rem(row, ROWS) // CAP * EIGHTS + row // ROWS * CAP + slot
            gather[rows] = (to == col).astype(BF16)
            return 0

        lax.fori_loop(0, 4, fill, 0)

    def split_weights():
        experts = lax.broadcasted_iota(jnp.int32, (128, EXPERTS), 1)
        hits = [experts == ids[:, k : k + 1] for k in range(2)]
        member = (hits[0] | hits[1]).astype(BF16)
        before = lax.broadcasted_iota(jnp.int32, (128, 128), 1) < lax.broadcasted_iota(jnp.int32, (128, 128), 0)
        earlier = jnp.dot(before.astype(BF16), member, preferred_element_type=F32)
        col = lax.broadcasted_iota(jnp.int32, (128, ROWS), 1)
        for x in range(LOCAL):
            total = jnp.zeros((128, ROWS), F32)
            for k in range(2):
                place = jnp.sum(jnp.where(hits[k], earlier, 0.0), axis=1, keepdims=True).astype(jnp.int32)
                one = ids[:, k : k + 1]
                here = (one & 1 == x) & ((one >> 1) * CAP + place == col)
                total = total + jnp.where(here, weights[:, k : k + 1], 0.0)
            high = total.astype(BF16)
            shares[x, 0:128] = high
            shares[x, 128:256] = (total - high.astype(F32)).astype(BF16)
    steps = (1, NZ - 1)

    def place(way, m):
        if m == STEPS:
            return z, way
        return lax.rem(z + SCATTER_D[m] * steps[way], NZ), SCATTER_X[way][m]

    def across(way, m):
        return remote(
            c_out.at[way, m], c_in.at[way, m], c_send.at[way, m], c_recv.at[way, m],
            (ep, z, 1 - core),
        )

    def ring_copy(way, m):
        return remote(
            r_out.at[way, m], r_in.at[way, m], r_send.at[way, m], r_recv.at[way, m],
            (ep, lax.rem(z + steps[way], NZ), core),
        )

    def partial(at, at_core, x, add, out):
        def tile(j, _):
            cols = pl.ds(pl.multiple_of(j * 512, 512), 512)
            total = jnp.dot(hid[at, at_core, x], w_down[x, :, cols], preferred_element_type=F32)
            for ref in add:
                total = total + ref[:, cols].astype(F32)
            out[:, cols] = total.astype(BF16)
            return 0

        lax.fori_loop(0, 4, tile, 0)

    def help_other(m):
        for way in range(2):
            at, x = place(way, m)
            partial(at, 1 - core, x, (), c_out.at[way, m])
            across(way, m).start()

    help_other(0)
    help_other(1)
    for m in range(STEPS):
        for way in range(2):
            at, x = place(way, m)
            add = [c_in.at[way, m]]
            across(way, m).wait_recv()
            came = SCATTER_IN[way][m]
            if came is not None:
                ring_copy(way, came).wait_recv()
                add.append(r_in.at[way, came])
            partial(at, core, x, add, r_out.at[way, m])
            ring_copy(way, m).start()
        if m + 2 <= STEPS:
            help_other(m + 2)
        if m == 0:
            split_weights()
        elif m == 1:
            tables()
        elif m < 5:
            lax.fori_loop((m - 2) * 5, (5, 10, 16)[m - 2], mix, 0)
        elif m == 6:
            lax.fori_loop(0, EP // 2, last, 0)

    def exchange(x, k):
        to = lax.rem(ep + k, EP)
        return remote(
            b_out.at[x, to], back.at[x, ep], a_send.at[x, k], a_recv.at[x, k], (to, z, core)
        )

    for x in (1, 0):
        across(x, STEPS).wait_recv()
        for way in range(2):
            ring_copy(way, LAST_IN[x][way]).wait_recv()

        def tile(j, _, x=x):
            cols = pl.ds(pl.multiple_of(j * 256, 256), 256)
            total = jnp.dot(hid[z, core, x], w_down[x, :, cols], preferred_element_type=F32)
            for ref in (c_in.at[x, STEPS], r_in.at[0, LAST_IN[x][0]], r_in.at[1, LAST_IN[x][1]]):
                total = total + ref[:, cols].astype(F32)
            b_in[j] = total.astype(BF16)
            return 0

        lax.fori_loop(0, 8, tile, 0)

        def spread_out(j, _, x=x):
            rows = pl.ds(pl.multiple_of(j * (4 * EIGHTS), 4 * EIGHTS), 4 * EIGHTS)
            wide = jnp.dot(spread[rows, :], b_in[...].reshape(8 * ROWS, 256), preferred_element_type=F32)
            b_out[x, pl.ds(j * 4, 4)] = wide.astype(BF16).reshape(4, EIGHTS, 256)
            return 0

        lax.fori_loop(0, 4, spread_out, 0)

        def send_one(k, _, x=x):
            exchange(x, k).start()
            return 0

        lax.fori_loop(1, EP, send_one, 0)
        back[x, ep] = b_out[x, ep]
    for x in (1, 0):

        def came_one(k, _, x=x):
            exchange(x, k).wait_recv()
            return 0

        lax.fori_loop(1, EP, came_one, 0)

        def combine(j, _, x=x):
            rows = pl.ds(pl.multiple_of(j * ROWS, ROWS), ROWS)
            part = jnp.dot(
                gather[rows], back[x].reshape(EP * EIGHTS, 256), preferred_element_type=F32
            ).astype(BF16)
            both = jnp.dot(shares[x], part, preferred_element_type=F32)
            both = both[0:128] + both[128:256]
            if x == 1:
                sums[j] = both
            else:
                cols = pl.ds(pl.multiple_of(j * 256, 256), 256)
                expert_out[:, cols] = (sums[j] + both).astype(BF16)
            return 0

        lax.fori_loop(0, 8, combine, 0)
    for way in range(2):
        for m in range(STEPS):
            ring_copy(way, m).wait_send()
            across(way, m).wait_send()
        across(way, STEPS).wait_send()
    for x in (1, 0):

        def end_one(k, _, x=x):
            exchange(x, k).wait_send()
            return 0

        lax.fori_loop(1, EP, end_one, 0)


DMA = pltpu.SemaphoreType.DMA


def per_device(
    mixer_in, expert_in, mixer_gain, w_outer, w_inner, w_value, conv_taps, w_mix_out,
    expert_gain, w_gate, w_up, w_down, route_ids, route_weights,
):
    tok_count, width = expert_in.shape
    taps = jnp.concatenate((conv_taps, jnp.zeros((5, 128), F32)), axis=0)
    vmem = pl.BlockSpec(memory_space=pltpu.VMEM)
    anywhere = pl.BlockSpec(memory_space=pl.ANY)
    hid, mix_rows, taps_all, wall = pl.pallas_call(
        gather_kernel,
        out_shape=(
            jax.ShapeDtypeStruct((NZ, 2, LOCAL, ROWS, 128), BF16),
            jax.ShapeDtypeStruct((tok_count + 16, width), BF16),
            jax.ShapeDtypeStruct((NZ * 2, 8, 128), F32),
            jax.ShapeDtypeStruct((EP, 2, NZ, 4, 128, 128), BF16),
        ),
        in_specs=[vmem] * 6 + [anywhere] * 6,
        out_specs=(vmem, vmem, vmem, anywhere),
        scratch_shapes=[
            pltpu.VMEM((512, 512), BF16),
            pltpu.VMEM((EP, QUADS, 512), BF16),
            pltpu.VMEM((EP, QUADS, 512), BF16),
            pltpu.VMEM((4, 128, 128), BF16),
            pltpu.VMEM((NZ, 4, 128, 128), BF16),
            pltpu.VMEM((16, width), BF16),
            pltpu.VMEM((16, width), BF16),
            pltpu.VMEM((LOCAL, ROWS, width), BF16),
            pltpu.VMEM((NZ, 2, LOCAL, ROWS, width), BF16),
            pltpu.VMEM((LOCAL, width, 256), BF16),
            DMA((4,)), DMA((LOCAL, 2)), DMA((EP,)), DMA((EP,)), DMA((2, STEPS)), DMA((2, STEPS)),
            DMA((NZ * 2,)), DMA((NZ * 2,)), DMA((2,)),
            DMA((2, STEPS)), DMA((2, STEPS)), DMA((2, STEPS + 1)), DMA((2, STEPS + 1)),
            DMA((2, 2, KINDS)), DMA((2, 2, KINDS)), DMA((2, 2, KINDS)), DMA((2, 2, KINDS)), DMA((3,)),
        ],
        cost_estimate=pl.CostEstimate(flops=10**11, bytes_accessed=3 * 10**8, transcendentals=0),
        compiler_params=pltpu.CompilerParams(
            collective_id=0, has_side_effects=True, vmem_limit_bytes=60 * 2**20
        ),
        name="gather_experts",
    )(
        mixer_in, expert_in, mixer_gain[None, :], expert_gain[None, :], route_ids.T, taps,
        w_outer, w_inner, w_value, w_mix_out, w_gate, w_up,
    )
    return pl.pallas_call(
        scatter_kernel,
        out_shape=(
            jax.ShapeDtypeStruct((tok_count, width), BF16),
            jax.ShapeDtypeStruct((tok_count, width), BF16),
        ),
        in_specs=[vmem] * 6 + [anywhere],
        out_specs=(vmem, vmem),
        scratch_shapes=[
            pltpu.VMEM((2, STEPS + 1, ROWS, width), BF16),
            pltpu.VMEM((2, STEPS + 1, ROWS, width), BF16),
            pltpu.VMEM((2, STEPS, ROWS, width), BF16),
            pltpu.VMEM((2, STEPS, ROWS, width), BF16),
            pltpu.VMEM((8, ROWS, 256), BF16),
            pltpu.VMEM((LOCAL, EP, EIGHTS, 256), BF16),
            pltpu.VMEM((LOCAL, EP, EIGHTS, 256), BF16),
            pltpu.VMEM((EP * EIGHTS, 8 * ROWS), BF16),
            pltpu.VMEM((8 * ROWS, EP * EIGHTS), BF16),
            pltpu.VMEM((LOCAL, 256, ROWS), BF16),
            pltpu.VMEM((8, 128, 256), F32),
            pltpu.VMEM((NZ * 2, 128, 128), BF16),
            pltpu.VMEM((2, EP, 3, 128, 128), BF16),
            pltpu.VMEM((2, 2, 2, NZ, 128, 128), BF16),
            DMA((2, STEPS + 1)), DMA((2, STEPS + 1)), DMA((2, STEPS)), DMA((2, STEPS)),
            DMA((LOCAL, EP)), DMA((LOCAL, EP)), DMA((2,)), DMA((2,)),
        ],
        cost_estimate=pl.CostEstimate(flops=10**11, bytes_accessed=3 * 10**8, transcendentals=0),
        compiler_params=pltpu.CompilerParams(
            collective_id=1, has_side_effects=True, vmem_limit_bytes=62 * 2**20
        ),
        name="scatter_experts",
    )(hid, w_down, mix_rows, taps_all, route_ids, route_weights, wall)


def solution(mesh):
    finer = Mesh(mesh.devices.reshape(mesh.shape["ep"], 8, 2), EP_TP)
    return jax.shard_map(
        per_device,
        mesh=finer,
        in_specs=(
            P(EP_TP, None), P(EP_TP, None), P(), P(None, TP), P(None, TP), P(None, TP),
            P(None, TP), P(TP, None), P(), P("ep", None, TP), P("ep", None, TP),
            P("ep", TP, None), P(EP_TP, None), P(EP_TP, None),
        ),
        out_specs=(P(EP_TP, None), P(EP_TP, None)),
        check_vma=False,
    )
```

```python
import functools

import jax
import jax.numpy as jnp
from jax import lax
from jax.experimental import pallas as pl
from jax.experimental.pallas import tpu as pltpu
from jax.sharding import Mesh
from jax.sharding import PartitionSpec as P

EXPERTS = 32
CAP = 10
EIGHTS = 80
EP = 16
NZ = 8
LOCAL = 2
ROWS = EP * CAP
TP = ("tp_0", "tp_1")
EP_TP = ("ep", "tp_0", "tp_1")
MESH = pl.DeviceIdType.MESH
F32 = jnp.float32
BF16 = jnp.bfloat16

norm_eps = 1e-06
clamp_limit = 7.0
gate_alpha = 1.702


def normed(values, gain):
    scaled = values * lax.rsqrt(jnp.mean(values * values, axis=-1, keepdims=True) + norm_eps)
    return (scaled * gain).astype(BF16)


def places():
    return lax.axis_index("ep"), lax.axis_index("tp_0"), lax.axis_index("tp_1")


def signal(where):
    pl.semaphore_signal(
        pltpu.get_barrier_semaphore(), inc=1, device_id=where, device_id_type=MESH
    )


def signal_all(count, where):
    def one(k, _):
        signal(where(k))
        return 0

    lax.fori_loop(1, count, one, 0)


def signal_ring(ep, z, core):
    for step in (1, NZ - 1):
        signal((ep, lax.rem(z + step, NZ), core))
    signal((ep, z, 1 - core))


def remote(src, dst, send, recv, where):
    return pltpu.make_async_remote_copy(
        src_ref=src, dst_ref=dst, send_sem=send, recv_sem=recv, device_id=where, device_id_type=MESH
    )


def each(count, act):
    def one(k, _):
        act(k)
        return 0

    lax.fori_loop(1, count, one, 0)


GATHER_D = (1, 1, 2, 2, 3, 3, 4)
GATHER_X = ((0, 1, 0, 1, 0, 1, 0), (0, 1, 0, 1, 0, 1, 1))
SCATTER_D = ((3, 4, 2, 3, 1, 2, 1), (3, 4, 3, 2, 2, 1, 1))
SCATTER_X = ((1, 0, 1, 0, 1, 0, 0), (0, 1, 1, 0, 1, 1, 0))
SCATTER_IN = ((None, None, 0, 1, 2, 3, 5), (None, None, 1, 0, 2, 4, 3))
LAST_IN = {1: (4, 5), 0: (6, 6)}
STEPS = 7
C_IN = 3
C_OUT = 2
R_OUT = 3
LINE = (0, 3, 1, 2)
KINDS = 10


def forwards(way, n):
    nxt = 6 if (way, n) == (1, 5) else n + 2
    if nxt < STEPS and GATHER_X[way][nxt] == GATHER_X[way][n] and GATHER_D[nxt] == GATHER_D[n] + 1:
        return nxt
    return None


def whole_kernel(
    mixer_in, expert_in, mixer_gain, expert_gain, ids, weights, taps, w_down,
    w_outer, w_inner, w_value, w_mix, w_gate, w_up,
    mixer_out, expert_out, wall,
    tap, slots, landed, back, b_in, wz, halo, mix_rows, taps_all, units, w_both, hid,
    c_out, c_in, r_out, r_in, spread, gather, shares, sums, gated, w_slots,
    w_sem, g_sem, a_send, a_recv, b_send, b_recv, z_send, z_recv, t_send, t_recv, h_sem,
    r_send, r_recv, c_send, c_recv, x_send, x_recv, d_send, d_recv, o_sem,
    s_send, s_recv, p_send, p_recv, m_sem, free_sem,
):
    ep, z, core = places()
    own = pl.ds(pl.multiple_of(ep * 128, 128), 128)
    loads = [
        pltpu.make_async_copy(w.at[own], wz.at[z, i], w_sem.at[i])
        for i, w in enumerate((w_inner, w_value, w_outer))
    ]
    loads.append(pltpu.make_async_copy(w_mix.at[:, own], wz.at[z, 3], w_sem.at[3]))
    for load in loads:
        load.start()
    gate_loads = []
    for x in range(LOCAL):
        gate_loads.append(pltpu.make_async_copy(w_gate.at[x], w_both.at[x, :, 0:128], g_sem.at[x, 0]))
        gate_loads.append(pltpu.make_async_copy(w_up.at[x], w_both.at[x, :, 128:256], g_sem.at[x, 1]))
    for load in gate_loads:
        load.start()
    spot = z * 2 + core
    partner = (ep, z, 1 - core)

    def tp_peer(k):
        to = lax.rem(spot + k, NZ * 2)
        return ep, to // 2, lax.rem(to, 2)

    def in_order(step):
        to = lax.rem(ep * (NZ * 2) + spot + step, EP * NZ * 2)
        return to // (NZ * 2), lax.rem(to // 2, NZ), lax.rem(to, 2)

    def ep_peer(k):
        return lax.rem(ep + k, EP), z, core

    signal_all(EP, ep_peer)
    signal_all(NZ * 2, tp_peer)
    signal(in_order(1))
    signal(in_order(EP * NZ * 2 - 1))

    def exchange(x, k):
        where = ep_peer(k)
        return remote(
            slots.at[x, where[0]], landed.at[x, ep], a_send.at[x, k], a_recv.at[x, k], where
        )

    def hand_back(x, k):
        where = ep_peer(k)
        return remote(
            slots.at[x, where[0]], back.at[x, ep], b_send.at[x, k], b_recv.at[x, k], where
        )

    def tell_taps(k):
        return remote(tap, taps_all.at[spot], t_send.at[k], t_recv.at[k], tp_peer(k))

    def tell_tail():
        return remote(mix_rows.at[128:144], halo, h_sem.at[0], h_sem.at[1], in_order(1))

    steps = (NZ - 1, 1)

    def spread_z(way, n):
        away = GATHER_D[n] - 1
        at = lax.rem(z + away * steps[way], NZ)
        there = (ep, lax.rem(z + (NZ - steps[way]), NZ), core)
        two = pl.ds(2 * GATHER_X[way][n], 2)
        return remote(
            wz.at[at, two], wz.at[at, two], z_send.at[way, n], z_recv.at[way, n], there
        )

    def ring_copy(way, n):
        at = lax.rem(z + (GATHER_D[n] - 1) * steps[way], NZ)
        x = GATHER_X[way][n]
        there = lax.rem(z + (NZ - steps[way]), NZ)
        ref = units.at[at, core, x]
        return remote(ref, ref, r_send.at[way, n], r_recv.at[way, n], (ep, there, core))

    def across(way, n):
        mine = n == STEPS
        at = z if mine else lax.rem(z + GATHER_D[n] * steps[way], NZ)
        x = way if mine else GATHER_X[way][n]
        ref = units.at[at, core, x]
        return remote(ref, ref, c_send.at[way, n], c_recv.at[way, n], partner), at, x

    at_x, at_y = lax.rem(ep, 4), ep // 4

    def off(half, du, dv):
        dx, dy = (du, dv) if half == 0 else (dv, du)
        return lax.rem(at_y + dy, 4) * 4 + lax.rem(at_x + dx, 4)

    def piece(half, way, kind, e, at_core):
        zs = pl.ds(at_core * NZ + 4 * half, 4)
        if kind == 1 or kind >= 6:
            zs = pl.ds(at_core * NZ + 4 * half + 2 * way, 2)
        return wall.at[e, zs]

    def plane(half, way, kind):
        step = 1 if way == 0 else 3
        if kind == 0:
            e, to = ep, off(half, step, 0)
        elif kind == 1:
            e, to = off(half, 4 - step, 0), off(half, step, 0)
        elif kind < 6:
            e, to = off(half, LINE[kind - 2], 0), off(half, 0, step)
        else:
            e, to = off(half, LINE[kind - 6], 4 - step), off(half, 0, step)
        ref = piece(half, way, kind, e, core)
        return remote(
            wz.at[pl.ds(4 * half, 4)] if kind in (0, 2) else ref, ref,
            x_send.at[half, way, kind], x_recv.at[half, way, kind], (to, z, core),
        )

    def plane_over(half, way, kind):
        step = 1 if way == 0 else 3
        if kind == 0:
            e = off(half, 4 - step, 0)
        elif kind == 1:
            e = off(half, 2, 0)
        elif kind < 6:
            e = off(half, LINE[kind - 2], 4 - step)
        else:
            e = off(half, LINE[kind - 6], 2)
        ref = piece(half, way, kind, e, core)
        return remote(ref, ref, d_send.at[half, way, kind], d_recv.at[half, way, kind], partner)

    both_halves = [(half, way) for half in range(2) for way in range(2)]

    def take(*kinds):
        for kind in kinds:
            for half, way in both_halves:
                plane(half, way, kind).wait_recv()
                plane_over(half, way, kind).start()

    def give(*kinds):
        for kind in kinds:
            for half, way in both_halves:
                plane(half, way, kind).start()

    own_wall = wall.at[ep, pl.ds(core * NZ, NZ)]

    def own_over():
        return remote(wz, own_wall, o_sem.at[0], o_sem.at[1], partner)

    def own_keep():
        return pltpu.make_async_copy(wz, own_wall, o_sem.at[2])

    def compute(at_z, at_core, x):
        both = jnp.dot(units[at_z, at_core, x], w_both[x], preferred_element_type=F32)
        gate_pre = jnp.minimum(both[:, 0:128], clamp_limit)
        up_pre = jnp.clip(both[:, 128:256], -clamp_limit, clamp_limit)
        hid[at_z, at_core, x] = (
            (up_pre + 1.0) * gate_pre * jax.nn.sigmoid(gate_alpha * gate_pre)
        ).astype(BF16)

    def pass_z(n):
        for way in range(2):
            spread_z(way, n).wait_recv()
            nxt = forwards(way, n)
            if nxt is not None:
                spread_z(way, nxt).start()

    go = (1, NZ - 1)

    def place(way, m):
        if m == STEPS:
            return z, way
        return lax.rem(z + SCATTER_D[way][m] * go[way], NZ), SCATTER_X[way][m]

    def help_copy(way, m):
        return remote(
            c_out.at[way, m % C_OUT], c_in.at[way, m % C_IN], p_send.at[way, m], p_recv.at[way, m], partner
        )

    def sum_copy(way, m):
        return remote(
            r_out.at[way, m % R_OUT], r_in.at[way, m], s_send.at[way, m], s_recv.at[way, m],
            (ep, lax.rem(z + go[way], NZ), core),
        )

    def partial(at, at_core, x, add, out):
        def tile(j, _):
            cols = pl.ds(pl.multiple_of(j * 512, 512), 512)
            total = jnp.dot(hid[at, at_core, x], w_down[x, :, cols], preferred_element_type=F32)
            for ref in add:
                total = total + ref[:, cols].astype(F32)
            out[:, cols] = total.astype(BF16)
            return 0

        lax.fori_loop(0, 4, tile, 0)

    def help_other(m):
        for way in range(2):
            at, x = place(way, m)
            if m >= C_OUT:
                help_copy(way, m - C_OUT).wait_send()
            partial(at, 1 - core, x, (), c_out.at[way, m % C_OUT])
            if m >= C_IN:
                pl.semaphore_wait(free_sem.at[way], 1)
            help_copy(way, m).start()

    def used(way, m):
        if m + C_IN <= STEPS:
            pl.semaphore_signal(free_sem.at[way], inc=1, device_id=partner, device_id_type=MESH)

    def send_sums(m):
        for way in range(2):
            at, x = place(way, m)
            add = [c_in.at[way, m % C_IN]]
            help_copy(way, m).wait_recv()
            came = SCATTER_IN[way][m]
            if came is not None:
                sum_copy(way, came).wait_recv()
                add.append(r_in.at[way, came])
            if m >= R_OUT:
                sum_copy(way, m - R_OUT).wait_send()
            partial(at, core, x, add, r_out.at[way, m % R_OUT])
            sum_copy(way, m).start()
            used(way, m)

    def fetch(t):
        at = lax.rem(t, 2)
        return pltpu.make_async_copy(wall.at[:, t, 0:3], w_slots.at[at], m_sem.at[at, 0])

    def fetch_last(j):
        at = lax.rem(j, 2)
        return [
            pltpu.make_async_copy(wall.at[2 * j + i, :, 3], w_slots.at[at, :, i], m_sem.at[at, i])
            for i in range(2)
        ]

    def mix(t, _):
        fetch(t).wait()
        at = lax.rem(t, 2)
        rows = mix_rows[...]
        pair = jnp.concatenate([w_slots[at, :, i].reshape(2048, 128) for i in range(2)], axis=1)
        pair = jnp.dot(rows, pair, preferred_element_type=F32)
        prod = pair[:, 0:128] * pair[:, 128:256]
        outer = jnp.dot(
            rows[16:144], w_slots[at, :, 2].reshape(2048, 128), preferred_element_type=F32
        )
        tap_at = taps_all[lax.rem(t, NZ) * 2 + t // NZ]
        conv = tap_at[2:3] * prod[16:144] + tap_at[1:2] * prod[15:143] + tap_at[0:1] * prod[14:142]
        gated[t] = (outer * conv).astype(BF16)

        @pl.when(t + 2 < NZ * 2)
        def _():
            fetch(t + 2).start()

        return 0

    def last(j, _):
        for copy in fetch_last(j):
            copy.wait()
        at = lax.rem(j, 2)
        rows = jnp.concatenate([gated[t] for t in range(NZ * 2)], axis=1)
        pair = jnp.concatenate([w_slots[at, :, i].reshape(2048, 128) for i in range(2)], axis=1)
        cols = pl.ds(pl.multiple_of(j * 256, 256), 256)
        mixer_out[:, cols] = jnp.dot(rows, pair, preferred_element_type=F32).astype(BF16)

        @pl.when(j + 2 < EP // 2)
        def _():
            for copy in fetch_last(j + 2):
                copy.start()

        return 0

    def fill_tables(j, _):
        rows = pl.ds(pl.multiple_of(j * 320, 320), 320)
        row = lax.broadcasted_iota(jnp.int32, (320, 1), 0) + j * 320
        col = lax.broadcasted_iota(jnp.int32, (320, spread.shape[1]), 1)
        slot = lax.rem(row, CAP)
        to = lax.rem(row, EIGHTS) // CAP * ROWS + row // EIGHTS * CAP + slot
        spread[rows] = (to == col).astype(F32).astype(BF16)
        to = lax.rem(row, ROWS) // CAP * EIGHTS + row // ROWS * CAP + slot
        gather[rows] = (to == col).astype(F32).astype(BF16)
        return 0

    def spread_rows(x):
        def one(j, _):
            rows = pl.ds(pl.multiple_of(j * (4 * EIGHTS), 4 * EIGHTS), 4 * EIGHTS)
            wide = jnp.dot(spread[rows], b_in[...].reshape(8 * ROWS, 256), preferred_element_type=F32)
            slots[x, pl.ds(j * 4, 4)] = wide.astype(BF16).reshape(4, EIGHTS, 256)
            return 0

        lax.fori_loop(0, 4, one, 0)

    lax.fori_loop(0, 4, fill_tables, 0)
    experts = lax.broadcasted_iota(jnp.int32, (EXPERTS, 128), 0)
    hits = [experts == ids[k : k + 1, :] for k in range(2)]
    member = (hits[0] | hits[1]).astype(F32).astype(BF16)
    before = lax.broadcasted_iota(jnp.int32, (128, 128), 0) < lax.broadcasted_iota(jnp.int32, (128, 128), 1)
    earlier = jnp.dot(member, before.astype(F32).astype(BF16), preferred_element_type=F32)
    goes = []
    for k in range(2):
        slot = jnp.sum(jnp.where(hits[k], earlier, 0.0), axis=0, keepdims=True).astype(jnp.int32)
        one = ids[k : k + 1, :]
        goes.append((one & 1) * ROWS + (one >> 1) * CAP + slot)
    rows = normed(expert_in[...].astype(F32), expert_gain[...])
    slot_row = lax.broadcasted_iota(jnp.int32, (ROWS, 128), 0)
    for x in range(LOCAL):
        placing = (slot_row + x * ROWS == goes[0]) | (slot_row + x * ROWS == goes[1])
        placing = placing.astype(F32).astype(BF16)
        for j in range(8):
            cols = slice(j * 256, (j + 1) * 256)
            b_in[j] = jnp.dot(placing, rows[:, cols], preferred_element_type=F32).astype(BF16)
        spread_rows(x)
    pl.semaphore_wait(pltpu.get_barrier_semaphore(), EP + NZ * 2)
    each(EP, lambda k: exchange(0, k).start())
    for load in loads:
        load.wait()
    for n in range(LOCAL):
        for way in range(2):
            spread_z(way, n).start()
    each(EP, lambda k: exchange(1, k).start())
    tap[0:3] = taps[...]
    tap[3:8] = jnp.zeros((5, 128), F32)
    each(NZ * 2, lambda k: tell_taps(k).start())
    for x in range(LOCAL):
        landed[x, ep] = slots[x, ep]
    rows = normed(mixer_in[...].astype(F32), mixer_gain[...])
    mix_rows[16:144] = rows
    tell_tail().start()
    pass_z(0)
    taps_all[spot] = tap[...]
    slot_row = lax.broadcasted_iota(jnp.int32, (LOCAL * ROWS, 128), 0)
    held = jnp.zeros((LOCAL * ROWS, 128), F32)
    for k in range(2):
        held = held + jnp.where(slot_row == goes[k], weights[k : k + 1, :], 0.0)
    for x in range(LOCAL):
        total = held[x * ROWS : (x + 1) * ROWS].T
        high = total.astype(BF16)
        shares[x, 0:128] = high
        shares[x, 128:256] = (total - high.astype(F32)).astype(BF16)
    for n in range(1, 4):
        pass_z(n)

    def pack(x):
        def one(j, _):
            rows = pl.ds(pl.multiple_of(j * ROWS, ROWS), ROWS)
            cols = pl.ds(pl.multiple_of(j * 256, 256), 256)
            out = jnp.dot(
                gather[rows], landed[x].reshape(EP * EIGHTS, 256), preferred_element_type=F32
            )
            units[z, core, x, :, cols] = out.astype(BF16)
            return 0

        each(EP, lambda k: exchange(x, k).wait_recv())
        lax.fori_loop(0, 8, one, 0)
        for way in range(2):
            ring_copy(way, x).start()
        across(x, STEPS)[0].start()

    pack(0)
    for load in gate_loads:
        load.wait()
    compute(z, core, 0)
    for n in range(4, STEPS):
        pass_z(n)
    pack(1)
    give(0)
    give(2)
    own_over().start()
    own_keep().start()
    compute(z, core, 1)
    tell_tail().wait()
    lone = (ep == 0) & (spot == 0)
    mix_rows[0:16] = jnp.where(lone, jnp.zeros_like(halo), halo[...])
    each(NZ * 2, lambda k: tell_taps(k).wait())
    for x in range(LOCAL):
        copy, at, _ = across(x, STEPS)
        copy.wait_recv()
        compute(z, 1 - core, x)

    for n in range(STEPS):
        for way in range(2):
            ring_copy(way, n).wait_recv()
            nxt = forwards(way, n)
            if nxt is not None:
                ring_copy(way, nxt).start()
            across(way, n)[0].start()
        if n == 1:
            take(0)
            give(1, 3, 4)
        elif n == 2:
            take(2)
            give(6)
            take(1)
            give(5)
        elif n == 3:
            take(3)
            give(7)
        elif n == 4:
            take(4)
            give(8)
            take(6)
        for way in range(2):
            at = lax.rem(z + GATHER_D[n] * steps[way], NZ)
            compute(at, core, GATHER_X[way][n])
        for way in range(2):
            copy, at, x = across(way, n)
            copy.wait_recv()
            compute(at, 1 - core, x)
        if n == 4:
            each(EP, lambda k: exchange(0, k).wait_send())
            each(EP, lambda k: exchange(1, k).wait_send())
        elif n == 5:
            help_other(0)
            send_sums(0)
            take(5)
            give(9)
        elif n == 6:
            help_other(1)
            send_sums(1)
            help_other(2)
            take(7, 8)
    for m in range(2, STEPS):
        send_sums(m)
        help_other(m + 1)
        if m == 2:
            take(9)
            own_keep().wait()
            own_over().wait()
            for half, way in both_halves:
                for kind in range(KINDS):
                    plane(half, way, kind).wait_send()
                    plane_over(half, way, kind).wait()
            fetch(0).start()
            fetch(1).start()
            lax.fori_loop(0, 4, mix, 0)
        elif m == 3:
            lax.fori_loop(4, 10, mix, 0)
        elif m == 4:
            lax.fori_loop(10, NZ * 2, mix, 0)
            for j in range(2):
                for copy in fetch_last(j):
                    copy.start()
        elif m == 6:
            lax.fori_loop(0, EP // 2, last, 0)

    for x in (1, 0):
        help_copy(x, STEPS).wait_recv()
        for way in range(2):
            sum_copy(way, LAST_IN[x][way]).wait_recv()

        def tile(j, _, x=x):
            cols = pl.ds(pl.multiple_of(j * 256, 256), 256)
            total = jnp.dot(hid[z, core, x], w_down[x, :, cols], preferred_element_type=F32)
            for ref in (
                c_in.at[x, STEPS % C_IN], r_in.at[0, LAST_IN[x][0]], r_in.at[1, LAST_IN[x][1]]
            ):
                total = total + ref[:, cols].astype(F32)
            b_in[j] = total.astype(BF16)
            return 0

        lax.fori_loop(0, 8, tile, 0)
        spread_rows(x)
        each(EP, lambda k, x=x: hand_back(x, k).start())
        back[x, ep] = slots[x, ep]

    for x in (1, 0):
        each(EP, lambda k, x=x: hand_back(x, k).wait_recv())

        def combine(j, _, x=x):
            rows = pl.ds(pl.multiple_of(j * ROWS, ROWS), ROWS)
            values = jnp.dot(
                gather[rows], back[x].reshape(EP * EIGHTS, 256), preferred_element_type=F32
            ).astype(BF16)
            both = jnp.dot(shares[x], values, preferred_element_type=F32)
            both = both[0:128] + both[128:256]
            if x == 1:
                sums[j] = both
            else:
                cols = pl.ds(pl.multiple_of(j * 256, 256), 256)
                expert_out[:, cols] = (sums[j] + both).astype(BF16)
            return 0

        lax.fori_loop(0, 8, combine, 0)
    for way in range(2):
        for n in range(STEPS):
            spread_z(way, n).wait_send()
            ring_copy(way, n).wait_send()
            across(way, n)[0].wait_send()
        across(way, STEPS)[0].wait_send()
        for m in range(STEPS + 1 - C_OUT, STEPS + 1):
            help_copy(way, m).wait_send()
        for m in range(STEPS - R_OUT, STEPS):
            sum_copy(way, m).wait_send()
    for x in (1, 0):
        each(EP, lambda k, x=x: hand_back(x, k).wait_send())


DMA = pltpu.SemaphoreType.DMA


def per_device(
    mixer_in, expert_in, mixer_gain, w_outer, w_inner, w_value, conv_taps, w_mix_out,
    expert_gain, w_gate, w_up, w_down, route_ids, route_weights,
):
    tok_count, width = expert_in.shape
    vmem = pl.BlockSpec(memory_space=pltpu.VMEM)
    anywhere = pl.BlockSpec(memory_space=pl.ANY)
    out = jax.ShapeDtypeStruct((tok_count, width), BF16)
    mixer_out, expert_out, _ = pl.pallas_call(
        whole_kernel,
        out_shape=(out, out, jax.ShapeDtypeStruct((EP, 2 * NZ, 4, 128, 128), BF16)),
        in_specs=[vmem] * 8 + [anywhere] * 6,
        out_specs=(vmem, vmem, anywhere),
        scratch_shapes=[
            pltpu.VMEM((8, 128), F32),
            pltpu.VMEM((LOCAL, EP, EIGHTS, 256), BF16),
            pltpu.VMEM((LOCAL, EP, EIGHTS, 256), BF16),
            pltpu.VMEM((LOCAL, EP, EIGHTS, 256), BF16),
            pltpu.VMEM((8, ROWS, 256), BF16),
            pltpu.VMEM((NZ, 4, 128, 128), BF16),
            pltpu.VMEM((16, width), BF16),
            pltpu.VMEM((tok_count + 16, width), BF16),
            pltpu.VMEM((NZ * 2, 8, 128), F32),
            pltpu.VMEM((NZ, 2, LOCAL, ROWS, width), BF16),
            pltpu.VMEM((LOCAL, width, 256), BF16),
            pltpu.VMEM((NZ, 2, LOCAL, ROWS, 128), BF16),
            pltpu.VMEM((2, C_OUT, ROWS, width), BF16),
            pltpu.VMEM((2, C_IN, ROWS, width), BF16),
            pltpu.VMEM((2, R_OUT, ROWS, width), BF16),
            pltpu.VMEM((2, STEPS, ROWS, width), BF16),
            pltpu.VMEM((EP * EIGHTS, 8 * ROWS), BF16),
            pltpu.VMEM((8 * ROWS, EP * EIGHTS), BF16),
            pltpu.VMEM((LOCAL, 256, ROWS), BF16),
            pltpu.VMEM((8, 128, 256), F32),
            pltpu.VMEM((NZ * 2, 128, 128), BF16),
            pltpu.VMEM((2, EP, 3, 128, 128), BF16),
            DMA((4,)), DMA((LOCAL, 2)), DMA((LOCAL, EP)), DMA((LOCAL, EP)), DMA((LOCAL, EP)), DMA((LOCAL, EP)),
            DMA((2, STEPS)), DMA((2, STEPS)), DMA((NZ * 2,)), DMA((NZ * 2,)), DMA((2,)),
            DMA((2, STEPS)), DMA((2, STEPS)), DMA((2, STEPS + 1)), DMA((2, STEPS + 1)),
            DMA((2, 2, KINDS)), DMA((2, 2, KINDS)), DMA((2, 2, KINDS)), DMA((2, 2, KINDS)), DMA((3,)),
            DMA((2, STEPS)), DMA((2, STEPS)), DMA((2, STEPS + 1)), DMA((2, STEPS + 1)), DMA((2, 2)),
            pltpu.SemaphoreType.REGULAR((2,)),
        ],
        cost_estimate=pl.CostEstimate(flops=10**11, bytes_accessed=3 * 10**8, transcendentals=0),
        compiler_params=pltpu.CompilerParams(
            collective_id=0, has_side_effects=True, vmem_limit_bytes=67043328
        ),
        name="whole_block",
    )(
        mixer_in, expert_in, mixer_gain[None, :], expert_gain[None, :], route_ids.T, route_weights.T,
        conv_taps, w_down, w_outer, w_inner, w_value, w_mix_out, w_gate, w_up,
    )
    return mixer_out, expert_out


def solution(mesh):
    finer = Mesh(mesh.devices.reshape(mesh.shape["ep"], 8, 2), EP_TP)
    return jax.shard_map(
        per_device,
        mesh=finer,
        in_specs=(
            P(EP_TP, None), P(EP_TP, None), P(), P(None, TP), P(None, TP), P(None, TP),
            P(None, TP), P(TP, None), P(), P("ep", None, TP), P("ep", None, TP),
            P("ep", TP, None), P(EP_TP, None), P(EP_TP, None),
        ),
        out_specs=(P(EP_TP, None), P(EP_TP, None)),
        check_vma=False,
    )
```

```python
import functools

import jax
import jax.numpy as jnp
from jax import lax
from jax.experimental import pallas as pl
from jax.experimental.pallas import tpu as pltpu
from jax.sharding import Mesh
from jax.sharding import PartitionSpec as P

EXPERTS = 32
CAP = 10
EIGHTS = 80
EP = 16
NZ = 8
LOCAL = 2
ROWS = EP * CAP
TP = ("tp_0", "tp_1")
EP_TP = ("ep", "tp_0", "tp_1")
MESH = pl.DeviceIdType.MESH
F32 = jnp.float32
BF16 = jnp.bfloat16

norm_eps = 1e-06
clamp_limit = 7.0
gate_alpha = 1.702


def normed(values, gain):
    scaled = values * lax.rsqrt(jnp.mean(values * values, axis=-1, keepdims=True) + norm_eps)
    return (scaled * gain).astype(BF16)


def places():
    return lax.axis_index("ep"), lax.axis_index("tp_0"), lax.axis_index("tp_1")


def signal(where):
    pl.semaphore_signal(
        pltpu.get_barrier_semaphore(), inc=1, device_id=where, device_id_type=MESH
    )


def signal_all(count, where):
    def one(k, _):
        signal(where(k))
        return 0

    lax.fori_loop(1, count, one, 0)


def signal_ring(ep, z, core):
    for step in (1, NZ - 1):
        signal((ep, lax.rem(z + step, NZ), core))
    signal((ep, z, 1 - core))


def remote(src, dst, send, recv, where):
    return pltpu.make_async_remote_copy(
        src_ref=src, dst_ref=dst, send_sem=send, recv_sem=recv, device_id=where, device_id_type=MESH
    )


def each(count, act):
    def one(k, _):
        act(k)
        return 0

    lax.fori_loop(1, count, one, 0)


GATHER_D = (1, 1, 2, 2, 3, 3, 4)
GATHER_X = ((0, 1, 0, 1, 0, 1, 0), (0, 1, 0, 1, 0, 1, 1))
SCATTER_D = ((3, 4, 2, 3, 1, 2, 1), (3, 4, 3, 2, 2, 1, 1))
SCATTER_X = ((1, 0, 1, 0, 1, 0, 0), (0, 1, 1, 0, 1, 1, 0))
SCATTER_IN = ((None, None, 0, 1, 2, 3, 5), (None, None, 1, 0, 2, 4, 3))
LAST_IN = {1: (4, 5), 0: (6, 6)}
STEPS = 7
C_IN = 3
SWAP = 8 * EIGHTS
C_OUT = 2
R_OUT = 3
LINE = (0, 3, 1, 2)
KINDS = 10


def forwards(way, n):
    nxt = 6 if (way, n) == (1, 5) else n + 2
    if nxt < STEPS and GATHER_X[way][nxt] == GATHER_X[way][n] and GATHER_D[nxt] == GATHER_D[n] + 1:
        return nxt
    return None


def whole_kernel(
    expert_in, mixer_gain, expert_gain, ids, weights, taps,
    mixer_hbm, down_hbm, w_outer, w_inner, w_value, w_mix, w_gate, w_up,
    mixer_out, expert_out, wall,
    tap, slots, landed, back, b_in, wz, halo, mix_rows, taps_all, units, w_both, hid,
    mixer_in, w_down, c_out, c_in, r_out, r_in, swap, shares, sums, gated, w_slots,
    w_sem, g_sem, a_send, a_recv, b_send, b_recv, z_send, z_recv, t_send, t_recv, h_sem,
    r_send, r_recv, c_send, c_recv, x_send, x_recv, d_send, d_recv, o_sem,
    s_send, s_recv, p_send, p_recv, m_sem, i_sem, free_sem,
):
    ep, z, core = places()
    own = pl.ds(pl.multiple_of(ep * 128, 128), 128)
    loads = [
        pltpu.make_async_copy(w.at[own], wz.at[z, i], w_sem.at[i])
        for i, w in enumerate((w_inner, w_value, w_outer))
    ]
    loads.append(pltpu.make_async_copy(w_mix.at[:, own], wz.at[z, 3], w_sem.at[3]))
    for load in loads:
        load.start()
    gate_loads = []
    for x in range(LOCAL):
        gate_loads.append(pltpu.make_async_copy(w_gate.at[x], w_both.at[x, :, 0:128], g_sem.at[x, 0]))
        gate_loads.append(pltpu.make_async_copy(w_up.at[x], w_both.at[x, :, 128:256], g_sem.at[x, 1]))
    inputs = [
        pltpu.make_async_copy(mixer_hbm, mixer_in, i_sem.at[0]),
        pltpu.make_async_copy(down_hbm, w_down, i_sem.at[1]),
    ]
    for load in inputs + gate_loads:
        load.start()
    spot = z * 2 + core
    partner = (ep, z, 1 - core)

    def tp_peer(k):
        to = lax.rem(spot + k, NZ * 2)
        return ep, to // 2, lax.rem(to, 2)

    def in_order(step):
        to = lax.rem(ep * (NZ * 2) + spot + step, EP * NZ * 2)
        return to // (NZ * 2), lax.rem(to // 2, NZ), lax.rem(to, 2)

    def ep_peer(k):
        return lax.rem(ep + k, EP), z, core

    signal_all(EP, ep_peer)
    signal_all(NZ * 2, tp_peer)
    signal(in_order(1))
    signal(in_order(EP * NZ * 2 - 1))

    def exchange(x, k):
        where = ep_peer(k)
        return remote(
            slots.at[x, where[0]], landed.at[x, ep], a_send.at[x, k], a_recv.at[x, k], where
        )

    def hand_back(x, k):
        where = ep_peer(k)
        return remote(
            slots.at[x, where[0]], back.at[x, ep], b_send.at[x, k], b_recv.at[x, k], where
        )

    def tell_taps(k):
        return remote(tap, taps_all.at[spot], t_send.at[k], t_recv.at[k], tp_peer(k))

    def tell_tail():
        return remote(mix_rows.at[128:144], halo, h_sem.at[0], h_sem.at[1], in_order(1))

    steps = (NZ - 1, 1)

    def spread_z(way, n):
        away = GATHER_D[n] - 1
        at = lax.rem(z + away * steps[way], NZ)
        there = (ep, lax.rem(z + (NZ - steps[way]), NZ), core)
        two = pl.ds(2 * GATHER_X[way][n], 2)
        return remote(
            wz.at[at, two], wz.at[at, two], z_send.at[way, n], z_recv.at[way, n], there
        )

    def ring_copy(way, n):
        at = lax.rem(z + (GATHER_D[n] - 1) * steps[way], NZ)
        x = GATHER_X[way][n]
        there = lax.rem(z + (NZ - steps[way]), NZ)
        ref = units.at[at, core, x]
        return remote(ref, ref, r_send.at[way, n], r_recv.at[way, n], (ep, there, core))

    def across(way, n):
        mine = n == STEPS
        at = z if mine else lax.rem(z + GATHER_D[n] * steps[way], NZ)
        x = way if mine else GATHER_X[way][n]
        ref = units.at[at, core, x]
        return remote(ref, ref, c_send.at[way, n], c_recv.at[way, n], partner), at, x

    at_x, at_y = lax.rem(ep, 4), ep // 4

    def off(half, du, dv):
        dx, dy = (du, dv) if half == 0 else (dv, du)
        return lax.rem(at_y + dy, 4) * 4 + lax.rem(at_x + dx, 4)

    def piece(half, way, kind, e, at_core):
        zs = pl.ds(at_core * NZ + 4 * half, 4)
        if kind == 1 or kind >= 6:
            zs = pl.ds(at_core * NZ + 4 * half + 2 * way, 2)
        return wall.at[e, zs]

    def plane(half, way, kind):
        step = 1 if way == 0 else 3
        if kind == 0:
            e, to = ep, off(half, step, 0)
        elif kind == 1:
            e, to = off(half, 4 - step, 0), off(half, step, 0)
        elif kind < 6:
            e, to = off(half, LINE[kind - 2], 0), off(half, 0, step)
        else:
            e, to = off(half, LINE[kind - 6], 4 - step), off(half, 0, step)
        ref = piece(half, way, kind, e, core)
        return remote(
            wz.at[pl.ds(4 * half, 4)] if kind in (0, 2) else ref, ref,
            x_send.at[half, way, kind], x_recv.at[half, way, kind], (to, z, core),
        )

    def plane_over(half, way, kind):
        step = 1 if way == 0 else 3
        if kind == 0:
            e = off(half, 4 - step, 0)
        elif kind == 1:
            e = off(half, 2, 0)
        elif kind < 6:
            e = off(half, LINE[kind - 2], 4 - step)
        else:
            e = off(half, LINE[kind - 6], 2)
        ref = piece(half, way, kind, e, core)
        return remote(ref, ref, d_send.at[half, way, kind], d_recv.at[half, way, kind], partner)

    both_halves = [(half, way) for half in range(2) for way in range(2)]

    def take(*kinds):
        for kind in kinds:
            for half, way in both_halves:
                plane(half, way, kind).wait_recv()
                plane_over(half, way, kind).start()

    def give(*kinds):
        for kind in kinds:
            for half, way in both_halves:
                plane(half, way, kind).start()

    own_wall = wall.at[ep, pl.ds(core * NZ, NZ)]

    def own_over():
        return remote(wz, own_wall, o_sem.at[0], o_sem.at[1], partner)

    def own_keep():
        return pltpu.make_async_copy(wz, own_wall, o_sem.at[2])

    def compute(at_z, at_core, x):
        both = jnp.dot(units[at_z, at_core, x], w_both[x], preferred_element_type=F32)
        gate_pre = jnp.minimum(both[:, 0:128], clamp_limit)
        up_pre = jnp.clip(both[:, 128:256], -clamp_limit, clamp_limit)
        hid[at_z, at_core, x] = (
            (up_pre + 1.0) * gate_pre * jax.nn.sigmoid(gate_alpha * gate_pre)
        ).astype(BF16)

    def pass_z(n):
        for way in range(2):
            spread_z(way, n).wait_recv()
            nxt = forwards(way, n)
            if nxt is not None:
                spread_z(way, nxt).start()

    go = (1, NZ - 1)

    def place(way, m):
        if m == STEPS:
            return z, way
        return lax.rem(z + SCATTER_D[way][m] * go[way], NZ), SCATTER_X[way][m]

    def help_copy(way, m):
        return remote(
            c_out.at[way, m % C_OUT], c_in.at[way, m % C_IN], p_send.at[way, m], p_recv.at[way, m], partner
        )

    def sum_copy(way, m):
        return remote(
            r_out.at[way, m % R_OUT], r_in.at[way, m], s_send.at[way, m], s_recv.at[way, m],
            (ep, lax.rem(z + go[way], NZ), core),
        )

    def partial(at, at_core, x, add, out):
        def tile(j, _):
            cols = pl.ds(pl.multiple_of(j * 512, 512), 512)
            total = jnp.dot(hid[at, at_core, x], w_down[x, :, cols], preferred_element_type=F32)
            for ref in add:
                total = total + ref[:, cols].astype(F32)
            out[:, cols] = total.astype(BF16)
            return 0

        lax.fori_loop(0, 4, tile, 0)

    def help_other(m):
        for way in range(2):
            at, x = place(way, m)
            if m >= C_OUT:
                help_copy(way, m - C_OUT).wait_send()
            partial(at, 1 - core, x, (), c_out.at[way, m % C_OUT])
            if m >= C_IN:
                pl.semaphore_wait(free_sem.at[way], 1)
            help_copy(way, m).start()

    def used(way, m):
        if m + C_IN <= STEPS:
            pl.semaphore_signal(free_sem.at[way], inc=1, device_id=partner, device_id_type=MESH)

    def send_sum(way, m):
        at, x = place(way, m)
        add = [c_in.at[way, m % C_IN]]
        help_copy(way, m).wait_recv()
        came = SCATTER_IN[way][m]
        if came is not None:
            sum_copy(way, came).wait_recv()
            add.append(r_in.at[way, came])
        if m >= R_OUT:
            sum_copy(way, m - R_OUT).wait_send()
        partial(at, core, x, add, r_out.at[way, m % R_OUT])
        sum_copy(way, m).start()
        used(way, m)

    def fetch(t):
        at = lax.rem(t, 2)
        return pltpu.make_async_copy(wall.at[:, t, 0:3], w_slots.at[at], m_sem.at[at, 0])

    def fetch_last(j):
        at = lax.rem(j, 2)
        return [
            pltpu.make_async_copy(wall.at[2 * j + i, :, 3], w_slots.at[at, :, i], m_sem.at[at, i])
            for i in range(2)
        ]

    def mix(t, _):
        fetch(t).wait()
        at = lax.rem(t, 2)
        rows = mix_rows[...]
        pair = jnp.concatenate([w_slots[at, :, i].reshape(2048, 128) for i in range(2)], axis=1)
        pair = jnp.dot(rows, pair, preferred_element_type=F32)
        prod = pair[:, 0:128] * pair[:, 128:256]
        outer = jnp.dot(
            rows[16:144], w_slots[at, :, 2].reshape(2048, 128), preferred_element_type=F32
        )
        tap_at = taps_all[lax.rem(t, NZ) * 2 + t // NZ]
        conv = tap_at[2:3] * prod[16:144] + tap_at[1:2] * prod[15:143] + tap_at[0:1] * prod[14:142]
        gated[t] = (outer * conv).astype(BF16)

        @pl.when(t + 2 < NZ * 2)
        def _():
            fetch(t + 2).start()

        return 0

    def last(j, _):
        for copy in fetch_last(j):
            copy.wait()
        at = lax.rem(j, 2)
        rows = jnp.concatenate([gated[t] for t in range(NZ * 2)], axis=1)
        pair = jnp.concatenate([w_slots[at, :, i].reshape(2048, 128) for i in range(2)], axis=1)
        cols = pl.ds(pl.multiple_of(j * 256, 256), 256)
        mixer_out[:, cols] = jnp.dot(rows, pair, preferred_element_type=F32).astype(BF16)

        @pl.when(j + 2 < EP // 2)
        def _():
            for copy in fetch_last(j + 2):
                copy.start()

        return 0

    def fill_swap(j, _):
        rows = pl.ds(pl.multiple_of(j * 320, 320), 320)
        row = lax.broadcasted_iota(jnp.int32, (320, 1), 0) + j * 320
        col = lax.broadcasted_iota(jnp.int32, (320, SWAP), 1)
        to = lax.rem(row, EIGHTS) // CAP * EIGHTS + row // EIGHTS * CAP + lax.rem(row, CAP)
        swap[rows] = (to == col).astype(F32).astype(BF16)
        return 0

    def spread_rows(x):
        def one(j, _):
            rows = pl.ds(pl.multiple_of(j * EIGHTS, EIGHTS), EIGHTS)
            wide = jnp.dot(swap[...], b_in[:, rows].reshape(SWAP, 256), preferred_element_type=F32)
            slots[x, pl.ds(j * 8, 8)] = wide.astype(BF16).reshape(8, EIGHTS, 256)
            return 0

        lax.fori_loop(0, 2, one, 0)

    def gather_rows(got):
        def one(j, _):
            rows = pl.ds(pl.multiple_of(j * EIGHTS, EIGHTS), EIGHTS)
            out = jnp.dot(swap[...], got[pl.ds(j * 8, 8)].reshape(SWAP, 256), preferred_element_type=F32)
            b_in[:, rows] = out.astype(BF16).reshape(8, EIGHTS, 256)
            return 0

        lax.fori_loop(0, 2, one, 0)

    rows = normed(expert_in[...].astype(F32), expert_gain[...])
    experts = lax.broadcasted_iota(jnp.int32, (EXPERTS, 128), 0)
    hits = [experts == ids[k : k + 1, :] for k in range(2)]
    member = (hits[0] | hits[1]).astype(F32).astype(BF16)
    before = lax.broadcasted_iota(jnp.int32, (128, 128), 0) < lax.broadcasted_iota(jnp.int32, (128, 128), 1)
    earlier = jnp.dot(member, before.astype(F32).astype(BF16), preferred_element_type=F32)
    goes = []
    for k in range(2):
        slot = jnp.sum(jnp.where(hits[k], earlier, 0.0), axis=0, keepdims=True).astype(jnp.int32)
        one = ids[k : k + 1, :]
        goes.append((one & 1) * ROWS + (one >> 1) * CAP + slot)
    slot_row = lax.broadcasted_iota(jnp.int32, (ROWS, 128), 0)

    def fill_slots(x):
        placing = (slot_row + x * ROWS == goes[0]) | (slot_row + x * ROWS == goes[1])
        out = jnp.dot(placing.astype(F32).astype(BF16), rows, preferred_element_type=F32).astype(BF16)
        for j in range(8):
            b_in[j] = out[:, j * 256 : (j + 1) * 256]
        spread_rows(x)

    pl.semaphore_wait(pltpu.get_barrier_semaphore(), EP + NZ * 2)
    for load in loads:
        load.wait()
    for n in range(LOCAL):
        for way in range(2):
            spread_z(way, n).start()
    lax.fori_loop(0, 2, fill_swap, 0)
    fill_slots(0)
    each(EP, lambda k: exchange(0, k).start())
    pass_z(0)
    fill_slots(1)
    each(EP, lambda k: exchange(1, k).start())
    pass_z(1)
    for x in range(LOCAL):
        landed[x, ep] = slots[x, ep]
    tap[0:3] = taps[...]
    tap[3:8] = jnp.zeros((5, 128), F32)
    each(NZ * 2, lambda k: tell_taps(k).start())
    for load in inputs:
        load.wait()
    mixed = normed(mixer_in[...].astype(F32), mixer_gain[...])
    mix_rows[16:144] = mixed
    pass_z(2)
    tell_tail().start()
    taps_all[spot] = tap[...]
    slot_row = lax.broadcasted_iota(jnp.int32, (LOCAL * ROWS, 128), 0)
    held = jnp.zeros((LOCAL * ROWS, 128), F32)
    for k in range(2):
        held = held + jnp.where(slot_row == goes[k], weights[k : k + 1, :], 0.0)
    pass_z(3)
    for x in range(LOCAL):
        total = held[x * ROWS : (x + 1) * ROWS].T
        high = total.astype(BF16)
        shares[x, 0:128] = high
        shares[x, 128:256] = (total - high.astype(F32)).astype(BF16)
    for load in gate_loads:
        load.wait()
    for n in range(4, STEPS):
        pass_z(n)

    def pack(x):
        each(EP, lambda k: exchange(x, k).wait_recv())
        gather_rows(landed.at[x])
        for j in range(8):
            units[z, core, x, :, j * 256 : (j + 1) * 256] = b_in[j]
        for way in range(2):
            ring_copy(way, x).start()
        across(x, STEPS)[0].start()

    pack(0)
    compute(z, core, 0)
    pack(1)
    give(0)
    give(2)
    own_over().start()
    own_keep().start()
    compute(z, core, 1)
    tell_tail().wait()
    lone = (ep == 0) & (spot == 0)
    mix_rows[0:16] = jnp.where(lone, jnp.zeros_like(halo), halo[...])
    each(NZ * 2, lambda k: tell_taps(k).wait())
    for x in range(LOCAL):
        copy, at, _ = across(x, STEPS)
        copy.wait_recv()
        compute(z, 1 - core, x)

    for n in range(STEPS):
        for way in range(2):
            ring_copy(way, n).wait_recv()
            nxt = forwards(way, n)
            if nxt is not None:
                ring_copy(way, nxt).start()
            across(way, n)[0].start()
        if n == 1:
            take(0)
            give(1, 3, 4)
        elif n == 2:
            take(2)
            give(6)
            take(1)
            give(5)
        elif n == 3:
            take(3)
            give(7)
        elif n == 4:
            take(4)
            give(8)
            take(6)
        for way in range(2):
            at = lax.rem(z + GATHER_D[n] * steps[way], NZ)
            compute(at, core, GATHER_X[way][n])
        for way in range(2):
            copy, at, x = across(way, n)
            copy.wait_recv()
            compute(at, 1 - core, x)
        if n == 4:
            each(EP, lambda k: exchange(0, k).wait_send())
            each(EP, lambda k: exchange(1, k).wait_send())
        elif n == 5:
            help_other(0)
            send_sum(1, 0)
            send_sum(0, 0)
            take(5)
            give(9)
        elif n == 6:
            help_other(1)
            send_sum(0, 1)
            send_sum(1, 1)
            help_other(2)
            take(7, 8)
    take(9)
    own_keep().wait()
    own_over().wait()
    for half, way in both_halves:
        for kind in range(KINDS):
            plane(half, way, kind).wait_send()
            plane_over(half, way, kind).wait()
    fetch(0).start()
    fetch(1).start()
    send_sum(0, 2)
    lax.fori_loop(0, 6, mix, 0)
    help_other(3)
    send_sum(1, 2)
    send_sum(0, 3)
    send_sum(1, 3)
    help_other(4)
    lax.fori_loop(6, 11, mix, 0)
    send_sum(0, 4)
    send_sum(1, 4)
    help_other(5)
    lax.fori_loop(11, NZ * 2, mix, 0)
    for j in range(2):
        for copy in fetch_last(j):
            copy.start()
    send_sum(0, 5)
    help_other(6)
    lax.fori_loop(0, EP // 2, last, 0)
    send_sum(1, 5)
    send_sum(0, 6)
    send_sum(1, 6)
    help_other(7)

    for x in (1, 0):
        help_copy(x, STEPS).wait_recv()
        for way in range(2):
            sum_copy(way, LAST_IN[x][way]).wait_recv()

        def tile(j, _, x=x):
            cols = pl.ds(pl.multiple_of(j * 256, 256), 256)
            total = jnp.dot(hid[z, core, x], w_down[x, :, cols], preferred_element_type=F32)
            for ref in (
                c_in.at[x, STEPS % C_IN], r_in.at[0, LAST_IN[x][0]], r_in.at[1, LAST_IN[x][1]]
            ):
                total = total + ref[:, cols].astype(F32)
            b_in[j] = total.astype(BF16)
            return 0

        lax.fori_loop(0, 8, tile, 0)
        spread_rows(x)
        each(EP, lambda k, x=x: hand_back(x, k).start())
        back[x, ep] = slots[x, ep]

    for x in (1, 0):
        each(EP, lambda k, x=x: hand_back(x, k).wait_recv())

        gather_rows(back.at[x])

        def combine(j, _, x=x):
            values = b_in[j]
            both = jnp.dot(shares[x], values, preferred_element_type=F32)
            both = both[0:128] + both[128:256]
            if x == 1:
                sums[j] = both
            else:
                cols = pl.ds(pl.multiple_of(j * 256, 256), 256)
                expert_out[:, cols] = (sums[j] + both).astype(BF16)
            return 0

        lax.fori_loop(0, 8, combine, 0)
    for way in range(2):
        for n in range(STEPS):
            spread_z(way, n).wait_send()
            ring_copy(way, n).wait_send()
            across(way, n)[0].wait_send()
        across(way, STEPS)[0].wait_send()
        for m in range(STEPS + 1 - C_OUT, STEPS + 1):
            help_copy(way, m).wait_send()
        for m in range(STEPS - R_OUT, STEPS):
            sum_copy(way, m).wait_send()
    for x in (1, 0):
        each(EP, lambda k, x=x: hand_back(x, k).wait_send())


DMA = pltpu.SemaphoreType.DMA


def per_device(
    mixer_in, expert_in, mixer_gain, w_outer, w_inner, w_value, conv_taps, w_mix_out,
    expert_gain, w_gate, w_up, w_down, route_ids, route_weights,
):
    tok_count, width = expert_in.shape
    vmem = pl.BlockSpec(memory_space=pltpu.VMEM)
    anywhere = pl.BlockSpec(memory_space=pl.ANY)
    out = jax.ShapeDtypeStruct((tok_count, width), BF16)
    mixer_out, expert_out, _ = pl.pallas_call(
        whole_kernel,
        out_shape=(out, out, jax.ShapeDtypeStruct((EP, 2 * NZ, 4, 128, 128), BF16)),
        in_specs=[vmem] * 6 + [anywhere] * 8,
        out_specs=(vmem, vmem, anywhere),
        scratch_shapes=[
            pltpu.VMEM((8, 128), F32),
            pltpu.VMEM((LOCAL, EP, EIGHTS, 256), BF16),
            pltpu.VMEM((LOCAL, EP, EIGHTS, 256), BF16),
            pltpu.VMEM((LOCAL, EP, EIGHTS, 256), BF16),
            pltpu.VMEM((8, ROWS, 256), BF16),
            pltpu.VMEM((NZ, 4, 128, 128), BF16),
            pltpu.VMEM((16, width), BF16),
            pltpu.VMEM((tok_count + 16, width), BF16),
            pltpu.VMEM((NZ * 2, 8, 128), F32),
            pltpu.VMEM((NZ, 2, LOCAL, ROWS, width), BF16),
            pltpu.VMEM((LOCAL, width, 256), BF16),
            pltpu.VMEM((NZ, 2, LOCAL, ROWS, 128), BF16),
            pltpu.VMEM((tok_count, width), BF16),
            pltpu.VMEM(w_down.shape, BF16),
            pltpu.VMEM((2, C_OUT, ROWS, width), BF16),
            pltpu.VMEM((2, C_IN, ROWS, width), BF16),
            pltpu.VMEM((2, R_OUT, ROWS, width), BF16),
            pltpu.VMEM((2, STEPS, ROWS, width), BF16),
            pltpu.VMEM((SWAP, SWAP), BF16),
            pltpu.VMEM((LOCAL, 256, ROWS), BF16),
            pltpu.VMEM((8, 128, 256), F32),
            pltpu.VMEM((NZ * 2, 128, 128), BF16),
            pltpu.VMEM((2, EP, 3, 128, 128), BF16),
            DMA((4,)), DMA((LOCAL, 2)), DMA((LOCAL, EP)), DMA((LOCAL, EP)), DMA((LOCAL, EP)), DMA((LOCAL, EP)),
            DMA((2, STEPS)), DMA((2, STEPS)), DMA((NZ * 2,)), DMA((NZ * 2,)), DMA((2,)),
            DMA((2, STEPS)), DMA((2, STEPS)), DMA((2, STEPS + 1)), DMA((2, STEPS + 1)),
            DMA((2, 2, KINDS)), DMA((2, 2, KINDS)), DMA((2, 2, KINDS)), DMA((2, 2, KINDS)), DMA((3,)),
            DMA((2, STEPS)), DMA((2, STEPS)), DMA((2, STEPS + 1)), DMA((2, STEPS + 1)), DMA((2, 2)), DMA((2,)),
            pltpu.SemaphoreType.REGULAR((2,)),
        ],
        cost_estimate=pl.CostEstimate(flops=10**11, bytes_accessed=3 * 10**8, transcendentals=0),
        compiler_params=pltpu.CompilerParams(
            collective_id=0, has_side_effects=True, vmem_limit_bytes=67043328
        ),
        name="whole_block",
    )(
        expert_in, mixer_gain[None, :], expert_gain[None, :], route_ids.T, route_weights.T, conv_taps,
        mixer_in, w_down, w_outer, w_inner, w_value, w_mix_out, w_gate, w_up,
    )
    return mixer_out, expert_out


def solution(mesh):
    finer = Mesh(mesh.devices.reshape(mesh.shape["ep"], 8, 2), EP_TP)
    return jax.shard_map(
        per_device,
        mesh=finer,
        in_specs=(
            P(EP_TP, None), P(EP_TP, None), P(), P(None, TP), P(None, TP), P(None, TP),
            P(None, TP), P(TP, None), P(), P("ep", None, TP), P("ep", None, TP),
            P("ep", TP, None), P(EP_TP, None), P(EP_TP, None),
        ),
        out_specs=(P(EP_TP, None), P(EP_TP, None)),
        check_vma=False,
    )
```

```python
import functools

import jax
import jax.numpy as jnp
from jax import lax
from jax.experimental import pallas as pl
from jax.experimental.pallas import tpu as pltpu
from jax.sharding import Mesh
from jax.sharding import PartitionSpec as P

EXPERTS = 32
CAP = 10
EIGHTS = 80
EP = 16
NZ = 8
LOCAL = 2
ROWS = EP * CAP
TP = ("tp_0", "tp_1")
EP_TP = ("ep", "tp_0", "tp_1")
MESH = pl.DeviceIdType.MESH
F32 = jnp.float32
BF16 = jnp.bfloat16

norm_eps = 1e-06
clamp_limit = 7.0
gate_alpha = 1.702


def normed(values, gain):
    scaled = values * lax.rsqrt(jnp.mean(values * values, axis=-1, keepdims=True) + norm_eps)
    return (scaled * gain).astype(BF16)


def places():
    return lax.axis_index("ep"), lax.axis_index("tp_0"), lax.axis_index("tp_1")


def signal(where):
    pl.semaphore_signal(
        pltpu.get_barrier_semaphore(), inc=1, device_id=where, device_id_type=MESH
    )


def signal_all(count, where):
    def one(k, _):
        signal(where(k))
        return 0

    lax.fori_loop(1, count, one, 0)


def signal_ring(ep, z, core):
    for step in (1, NZ - 1):
        signal((ep, lax.rem(z + step, NZ), core))
    signal((ep, z, 1 - core))


def remote(src, dst, send, recv, where):
    return pltpu.make_async_remote_copy(
        src_ref=src, dst_ref=dst, send_sem=send, recv_sem=recv, device_id=where, device_id_type=MESH
    )


def drain(ref, sem):
    pltpu.make_async_copy(ref, ref, sem).wait()


def each(count, act):
    def one(k, _):
        act(k)
        return 0

    lax.fori_loop(1, count, one, 0)


GATHER_D = (1, 1, 2, 2, 3, 3, 4)
GATHER_X = ((0, 1, 0, 1, 0, 1, 0), (0, 1, 0, 1, 0, 1, 1))
SCATTER_D = ((3, 4, 2, 3, 1, 2, 1), (3, 4, 3, 2, 2, 1, 1))
SCATTER_X = ((1, 0, 1, 0, 1, 0, 0), (0, 1, 1, 0, 1, 1, 0))
SCATTER_IN = ((None, None, 0, 1, 2, 3, 5), (None, None, 1, 0, 2, 4, 3))
LAST_IN = {(1, 0): (4, 5), (1, 1): (4, 5), (0, 0): (6, 6), (0, 1): (7, 7)}
STEPS = 7
C_IN = 3
SWAP = 8 * EIGHTS
C_OUT = 2
R_OUT = 3
LINE = (0, 3, 1, 2)
KINDS = 10


def forwards(way, n):
    nxt = 6 if (way, n) == (1, 5) else n + 2
    if nxt < STEPS and GATHER_X[way][nxt] == GATHER_X[way][n] and GATHER_D[nxt] == GATHER_D[n] + 1:
        return nxt
    return None


def whole_kernel(
    expert_hbm, mixer_gain_hbm, expert_gain_hbm, ids_hbm, weights_hbm, taps_hbm,
    mixer_hbm, down_hbm, w_outer, w_inner, w_value, w_mix, w_gate, w_up,
    mixer_out, expert_out, wall,
    expert_in, mixer_gain, expert_gain, ids, weights, tap, mixer_in, w_down,
    slots, landed, b_slots, back, b_in, b_half, wz, halo, mix_rows, taps_all, units, w_both, hid,
    c_out, c_in, r_out, r_in, swap, shares, sums, gated, w_slots,
    w_sem, g_sem, a_send, a_recv, b_send, b_recv, z_send, z_recv, t_send, t_recv, h_sem,
    r_send, r_recv, c_send, c_recv, x_send, x_recv, d_send, d_recv, o_sem,
    s_send, s_recv, p_send, p_recv, m_sem, i_sem, free_sem,
):
    ep, z, core = places()
    own = pl.ds(pl.multiple_of(ep * 128, 128), 128)
    for i, w in enumerate((w_inner, w_value, w_outer)):
        pltpu.make_async_copy(w.at[own], wz.at[z, i], w_sem.at[0]).start()
    pltpu.make_async_copy(w_mix.at[:, own], wz.at[z, 3], w_sem.at[0]).start()
    pairs = (
        (expert_hbm, expert_in), (expert_gain_hbm, expert_gain), (ids_hbm, ids),
        (weights_hbm, weights), (taps_hbm, tap.at[0:3]), (mixer_gain_hbm, mixer_gain),
        (mixer_hbm, mixer_in), (down_hbm, w_down),
    )
    inputs = [pltpu.make_async_copy(src, dst, i_sem.at[i]) for i, (src, dst) in enumerate(pairs)]
    for load in inputs:
        load.start()
    for x in range(LOCAL):
        pltpu.make_async_copy(w_gate.at[x], w_both.at[x, :, 0:128], g_sem.at[0]).start()
        pltpu.make_async_copy(w_up.at[x], w_both.at[x, :, 128:256], g_sem.at[0]).start()
    spot = z * 2 + core
    partner = (ep, z, 1 - core)

    def tp_peer(k):
        to = lax.rem(spot + k, NZ * 2)
        return ep, to // 2, lax.rem(to, 2)

    def in_order(step):
        to = lax.rem(ep * (NZ * 2) + spot + step, EP * NZ * 2)
        return to // (NZ * 2), lax.rem(to // 2, NZ), lax.rem(to, 2)

    def ep_peer(k):
        return lax.rem(ep + k, EP), z, core

    signal_all(EP, ep_peer)
    signal_all(NZ * 2, tp_peer)
    signal(in_order(1))
    signal(in_order(EP * NZ * 2 - 1))

    def exchange(x, k):
        where = ep_peer(k)
        return remote(
            slots.at[x, where[0]], landed.at[x, ep], a_send.at[x], a_recv.at[x], where
        )

    def hand_back(x, part, k):
        where = ep_peer(k)
        return remote(
            b_slots.at[x, part, where[0]], back.at[x, part, ep],
            b_send.at[x, part], b_recv.at[x, part], where,
        )

    def tell_taps(k):
        return remote(tap, taps_all.at[spot], t_send.at[0], t_recv.at[0], tp_peer(k))

    def tell_tail():
        return remote(mix_rows.at[128:144], halo, h_sem.at[0], h_sem.at[1], in_order(1))

    steps = (NZ - 1, 1)

    def spread_z(way, n):
        away = GATHER_D[n] - 1
        at = lax.rem(z + away * steps[way], NZ)
        there = (ep, lax.rem(z + (NZ - steps[way]), NZ), core)
        two = pl.ds(2 * GATHER_X[way][n], 2)
        return remote(
            wz.at[at, two], wz.at[at, two], z_send.at[way], z_recv.at[way, n], there
        )

    def ring_copy(way, n):
        at = lax.rem(z + (GATHER_D[n] - 1) * steps[way], NZ)
        x = GATHER_X[way][n]
        there = lax.rem(z + (NZ - steps[way]), NZ)
        ref = units.at[at, core, x]
        return remote(ref, ref, r_send.at[way], r_recv.at[way, n], (ep, there, core))

    def across(way, n):
        mine = n == STEPS
        at = z if mine else lax.rem(z + GATHER_D[n] * steps[way], NZ)
        x = way if mine else GATHER_X[way][n]
        ref = units.at[at, core, x]
        return remote(ref, ref, c_send.at[way], c_recv.at[way, n], partner), at, x

    at_x, at_y = lax.rem(ep, 4), ep // 4

    def off(half, du, dv):
        dx, dy = (du, dv) if half == 0 else (dv, du)
        return lax.rem(at_y + dy, 4) * 4 + lax.rem(at_x + dx, 4)

    def piece(half, way, kind, e, at_core):
        zs = pl.ds(at_core * NZ + 4 * half, 4)
        if kind == 1 or kind >= 6:
            zs = pl.ds(at_core * NZ + 4 * half + 2 * way, 2)
        return wall.at[e, zs]

    def plane(half, way, kind):
        step = 1 if way == 0 else 3
        if kind == 0:
            e, to = ep, off(half, step, 0)
        elif kind == 1:
            e, to = off(half, 4 - step, 0), off(half, step, 0)
        elif kind < 6:
            e, to = off(half, LINE[kind - 2], 0), off(half, 0, step)
        else:
            e, to = off(half, LINE[kind - 6], 4 - step), off(half, 0, step)
        ref = piece(half, way, kind, e, core)
        return remote(
            wz.at[pl.ds(4 * half, 4)] if kind in (0, 2) else ref, ref,
            x_send.at[kind], x_recv.at[kind], (to, z, core),
        )

    def plane_over(half, way, kind):
        step = 1 if way == 0 else 3
        if kind == 0:
            e = off(half, 4 - step, 0)
        elif kind == 1:
            e = off(half, 2, 0)
        elif kind < 6:
            e = off(half, LINE[kind - 2], 4 - step)
        else:
            e = off(half, LINE[kind - 6], 2)
        ref = piece(half, way, kind, e, core)
        return remote(ref, ref, d_send.at[kind], d_recv.at[kind], partner)

    both_halves = [(half, way) for half in range(2) for way in range(2)]

    def four(kind):
        return wall.at[0, 0 : (NZ if kind == 1 or kind >= 6 else 2 * NZ)]

    def take(*kinds):
        for kind in kinds:
            drain(four(kind), x_recv.at[kind])
            for half, way in both_halves:
                plane_over(half, way, kind).start()

    def give(*kinds):
        for kind in kinds:
            for half, way in both_halves:
                plane(half, way, kind).start()

    own_wall = wall.at[ep, pl.ds(core * NZ, NZ)]

    def own_over():
        return remote(wz, own_wall, o_sem.at[0], o_sem.at[1], partner)

    def own_keep():
        return pltpu.make_async_copy(wz, own_wall, o_sem.at[2])

    def compute(at_z, at_core, x):
        both = jnp.dot(units[at_z, at_core, x], w_both[x], preferred_element_type=F32)
        gate_pre = jnp.minimum(both[:, 0:128], clamp_limit)
        up_pre = jnp.clip(both[:, 128:256], -clamp_limit, clamp_limit)
        hid[at_z, at_core, x] = (
            (up_pre + 1.0) * gate_pre * jax.nn.sigmoid(gate_alpha * gate_pre)
        ).astype(BF16)

    def pass_z(n):
        for way in range(2):
            spread_z(way, n).wait_recv()
            nxt = forwards(way, n)
            if nxt is not None:
                spread_z(way, nxt).start()

    go = (1, NZ - 1)

    def place(way, m):
        if m == STEPS:
            return z, way
        return lax.rem(z + SCATTER_D[way][m] * go[way], NZ), SCATTER_X[way][m]

    def help_copy(way, m):
        return remote(
            c_out.at[way, m % C_OUT], c_in.at[way, m % C_IN], p_send.at[way, m], p_recv.at[way, m], partner
        )

    def sum_copy(way, m):
        cols = slice(0, 2048) if m < 6 else slice(1024 * (m - 6), 1024 * (m - 5))
        step = min(m, 6)
        return remote(
            r_out.at[way, step % R_OUT, :, cols], r_in.at[way, step, :, cols],
            s_send.at[way, m], s_recv.at[way, m], (ep, lax.rem(z + go[way], NZ), core),
        )

    def partial(at, at_core, x, add, out, tiles=(0, 4)):
        def tile(j, _):
            cols = pl.ds(pl.multiple_of(j * 512, 512), 512)
            total = jnp.dot(hid[at, at_core, x], w_down[x, :, cols], preferred_element_type=F32)
            for ref in add:
                total = total + ref[:, cols].astype(F32)
            out[:, cols] = total.astype(BF16)
            return 0

        lax.fori_loop(*tiles, tile, 0)

    def help_other(m):
        for way in range(2):
            at, x = place(way, m)
            if m >= C_OUT:
                help_copy(way, m - C_OUT).wait_send()
            partial(at, 1 - core, x, (), c_out.at[way, m % C_OUT])
            if m >= C_IN:
                pl.semaphore_wait(free_sem.at[way], 1)
            help_copy(way, m).start()

    def used(way, m):
        if m + C_IN <= STEPS:
            pl.semaphore_signal(free_sem.at[way], inc=1, device_id=partner, device_id_type=MESH)

    def send_sum(way, m):
        at, x = place(way, m)
        add = [c_in.at[way, m % C_IN]]
        help_copy(way, m).wait_recv()
        came = SCATTER_IN[way][m]
        if came is not None:
            sum_copy(way, came).wait_recv()
            add.append(r_in.at[way, came])
        if m >= R_OUT:
            sum_copy(way, m - R_OUT).wait_send()
        if m < 6:
            partial(at, core, x, add, r_out.at[way, m % R_OUT])
            sum_copy(way, m).start()
        else:
            for part in range(2):
                partial(at, core, x, add, r_out.at[way, m % R_OUT], (2 * part, 2 * part + 2))
                sum_copy(way, 6 + part).start()
        used(way, m)

    def fetch(t):
        at = lax.rem(t, 2)
        return pltpu.make_async_copy(wall.at[:, t, 0:3], w_slots.at[at], m_sem.at[at, 0])

    def fetch_last(j):
        at = lax.rem(j, 2)
        return [
            pltpu.make_async_copy(wall.at[2 * j + i, :, 3], w_slots.at[at, :, i], m_sem.at[at, i])
            for i in range(2)
        ]

    def mix(t, _):
        fetch(t).wait()
        at = lax.rem(t, 2)
        rows = mix_rows[...]
        pair = jnp.concatenate([w_slots[at, :, i].reshape(2048, 128) for i in range(2)], axis=1)
        pair = jnp.dot(rows, pair, preferred_element_type=F32)
        prod = pair[:, 0:128] * pair[:, 128:256]
        outer = jnp.dot(
            rows[16:144], w_slots[at, :, 2].reshape(2048, 128), preferred_element_type=F32
        )
        tap_at = taps_all[lax.rem(t, NZ) * 2 + t // NZ]
        conv = tap_at[2:3] * prod[16:144] + tap_at[1:2] * prod[15:143] + tap_at[0:1] * prod[14:142]
        gated[t] = (outer * conv).astype(BF16)

        @pl.when(t + 2 < NZ * 2)
        def _():
            fetch(t + 2).start()

        return 0

    def last(j, _):
        for copy in fetch_last(j):
            copy.wait()
        at = lax.rem(j, 2)
        rows = jnp.concatenate([gated[t] for t in range(NZ * 2)], axis=1)
        pair = jnp.concatenate([w_slots[at, :, i].reshape(2048, 128) for i in range(2)], axis=1)
        cols = pl.ds(pl.multiple_of(j * 256, 256), 256)
        mixer_out[:, cols] = jnp.dot(rows, pair, preferred_element_type=F32).astype(BF16)

        @pl.when(j + 2 < EP // 2)
        def _():
            for copy in fetch_last(j + 2):
                copy.start()

        return 0

    def fill_swap(j, _):
        rows = pl.ds(pl.multiple_of(j * 320, 320), 320)
        row = lax.broadcasted_iota(jnp.int32, (320, 1), 0) + j * 320
        col = lax.broadcasted_iota(jnp.int32, (320, SWAP), 1)
        to = lax.rem(row, EIGHTS) // CAP * EIGHTS + row // EIGHTS * CAP + lax.rem(row, CAP)
        swap[rows] = (to == col).astype(F32).astype(BF16)
        return 0

    def spread_rows(x):
        def one(j, _):
            rows = pl.ds(pl.multiple_of(j * EIGHTS, EIGHTS), EIGHTS)
            wide = jnp.dot(swap[...], b_in[:, rows].reshape(SWAP, 256), preferred_element_type=F32)
            slots[x, pl.ds(j * 8, 8)] = wide.astype(BF16).reshape(8, EIGHTS, 256)
            return 0

        lax.fori_loop(0, 2, one, 0)

    def gather_rows(got):
        def one(j, _):
            rows = pl.ds(pl.multiple_of(j * EIGHTS, EIGHTS), EIGHTS)
            out = jnp.dot(swap[...], got[pl.ds(j * 8, 8)].reshape(SWAP, 256), preferred_element_type=F32)
            b_in[:, rows] = out.astype(BF16).reshape(8, EIGHTS, 256)
            return 0

        lax.fori_loop(0, 2, one, 0)

    tap[3:8] = jnp.zeros((5, 128), F32)
    lax.fori_loop(0, 2, fill_swap, 0)
    for load in inputs[0:3]:
        load.wait()
    rows = normed(expert_in[...].astype(F32), expert_gain[...])
    experts = lax.broadcasted_iota(jnp.int32, (EXPERTS, 128), 0)
    hits = [experts == ids[k : k + 1, :] for k in range(2)]
    member = (hits[0] | hits[1]).astype(F32).astype(BF16)
    before = lax.broadcasted_iota(jnp.int32, (128, 128), 0) < lax.broadcasted_iota(jnp.int32, (128, 128), 1)
    earlier = jnp.dot(member, before.astype(F32).astype(BF16), preferred_element_type=F32)
    goes = []
    for k in range(2):
        slot = jnp.sum(jnp.where(hits[k], earlier, 0.0), axis=0, keepdims=True).astype(jnp.int32)
        one = ids[k : k + 1, :]
        goes.append((one & 1) * ROWS + (one >> 1) * CAP + slot)
    slot_row = lax.broadcasted_iota(jnp.int32, (ROWS, 128), 0)

    def fill_slots(x):
        placing = (slot_row + x * ROWS == goes[0]) | (slot_row + x * ROWS == goes[1])
        out = jnp.dot(placing.astype(F32).astype(BF16), rows, preferred_element_type=F32).astype(BF16)
        for j in range(8):
            b_in[j] = out[:, j * 256 : (j + 1) * 256]
        spread_rows(x)

    pl.semaphore_wait(pltpu.get_barrier_semaphore(), EP + NZ * 2)
    drain(wz.at[z], w_sem.at[0])
    for n in range(LOCAL):
        for way in range(2):
            spread_z(way, n).start()
    fill_slots(0)
    each(EP, lambda k: exchange(0, k).start())
    pass_z(0)
    fill_slots(1)
    each(EP, lambda k: exchange(1, k).start())
    pass_z(1)
    for x in range(LOCAL):
        landed[x, ep] = slots[x, ep]
    for load in inputs[3:]:
        load.wait()
    each(NZ * 2, lambda k: tell_taps(k).start())
    mixed = normed(mixer_in[...].astype(F32), mixer_gain[...])
    mix_rows[16:144] = mixed
    pass_z(2)
    tell_tail().start()
    taps_all[spot] = tap[...]
    slot_row = lax.broadcasted_iota(jnp.int32, (LOCAL * ROWS, 128), 0)
    held = jnp.zeros((LOCAL * ROWS, 128), F32)
    for k in range(2):
        held = held + jnp.where(slot_row == goes[k], weights[k : k + 1, :], 0.0)
    pass_z(3)
    for x in range(LOCAL):
        total = held[x * ROWS : (x + 1) * ROWS].T
        high = total.astype(BF16)
        shares[x, 0:128] = high
        shares[x, 128:256] = (total - high.astype(F32)).astype(BF16)
    drain(w_both, g_sem.at[0])
    for n in range(4, STEPS):
        pass_z(n)

    def pack(x):
        drain(landed.at[x, 0 : EP - 1], a_recv.at[x])
        gather_rows(landed.at[x])
        for j in range(8):
            units[z, core, x, :, j * 256 : (j + 1) * 256] = b_in[j]
        for way in range(2):
            ring_copy(way, x).start()
        across(x, STEPS)[0].start()

    pack(0)
    compute(z, core, 0)
    pack(1)
    give(0)
    give(2)
    own_over().start()
    own_keep().start()
    compute(z, core, 1)
    tell_tail().wait()
    lone = (ep == 0) & (spot == 0)
    mix_rows[0:16] = jnp.where(lone, jnp.zeros_like(halo), halo[...])
    drain(taps_all.at[0 : NZ * 2 - 1], t_recv.at[0])
    drain(taps_all.at[0 : NZ * 2 - 1], t_send.at[0])
    for x in range(LOCAL):
        copy, at, _ = across(x, STEPS)
        copy.wait_recv()
        compute(z, 1 - core, x)

    for n in range(STEPS):
        for way in range(2):
            ring_copy(way, n).wait_recv()
            nxt = forwards(way, n)
            if nxt is not None:
                ring_copy(way, nxt).start()
            across(way, n)[0].start()
        if n == 1:
            take(0)
            give(1, 3, 4)
        elif n == 2:
            take(2)
            give(6)
            take(1)
            give(5)
        elif n == 3:
            take(3)
            give(7)
        elif n == 4:
            take(4)
            give(8)
            take(6)
        for way in range(2):
            at = lax.rem(z + GATHER_D[n] * steps[way], NZ)
            compute(at, core, GATHER_X[way][n])
        for way in range(2):
            copy, at, x = across(way, n)
            copy.wait_recv()
            compute(at, 1 - core, x)
        if n == 5:
            help_other(0)
            send_sum(1, 0)
            send_sum(0, 0)
            take(5)
            give(9)
        elif n == 6:
            help_other(1)
            send_sum(0, 1)
            send_sum(1, 1)
            help_other(2)
            take(7, 8)
    take(9)
    own_keep().wait()
    own_over().wait()
    for kind in range(KINDS):
        for sem in (d_recv, d_send, x_send):
            drain(four(kind), sem.at[kind])
    fetch(0).start()
    fetch(1).start()
    send_sum(0, 2)
    lax.fori_loop(0, 6, mix, 0)
    help_other(3)
    send_sum(1, 2)
    send_sum(0, 3)
    send_sum(1, 3)
    help_other(4)
    lax.fori_loop(6, 11, mix, 0)
    send_sum(0, 4)
    send_sum(1, 4)
    help_other(5)
    lax.fori_loop(11, NZ * 2, mix, 0)
    for j in range(2):
        for copy in fetch_last(j):
            copy.start()
    send_sum(0, 5)
    help_other(6)
    lax.fori_loop(0, EP // 2, last, 0)
    send_sum(1, 5)
    send_sum(0, 6)
    send_sum(1, 6)
    help_other(7)

    for x, part in ((1, 0), (1, 1), (0, 0), (0, 1)):
        if part == 0:
            help_copy(x, STEPS).wait_recv()
        if part == 0 or x == 0:
            for way in range(2):
                sum_copy(way, LAST_IN[x, part][way]).wait_recv()

        def tile(j, _, x=x, part=part):
            cols = pl.ds(pl.multiple_of(part * 1024 + j * 256, 256), 256)
            total = jnp.dot(hid[z, core, x], w_down[x, :, cols], preferred_element_type=F32)
            for ref in (
                c_in.at[x, STEPS % C_IN],
                r_in.at[0, min(LAST_IN[x, part][0], 6)],
                r_in.at[1, min(LAST_IN[x, part][1], 6)],
            ):
                total = total + ref[:, cols].astype(F32)
            total = total.astype(BF16)
            b_half[2 * j] = total[:, 0:128]
            b_half[2 * j + 1] = total[:, 128:256]
            return 0

        lax.fori_loop(0, 4, tile, 0)

        def swap_out(j, _, x=x, part=part):
            rows = pl.ds(pl.multiple_of(j * EIGHTS, EIGHTS), EIGHTS)
            wide = jnp.dot(swap[...], b_half[:, rows].reshape(SWAP, 128), preferred_element_type=F32)
            b_slots[x, part, pl.ds(j * 8, 8)] = wide.astype(BF16).reshape(8, EIGHTS, 128)
            return 0

        lax.fori_loop(0, 2, swap_out, 0)
        each(EP, lambda k, x=x, part=part: hand_back(x, part, k).start())
        back[x, part, ep] = b_slots[x, part, ep]

    for x, part in ((1, 0), (1, 1), (0, 0), (0, 1)):
        drain(back.at[x, part, 0 : EP - 1], b_recv.at[x, part])

        def swap_in(j, _, x=x, part=part):
            rows = pl.ds(pl.multiple_of(j * EIGHTS, EIGHTS), EIGHTS)
            out = jnp.dot(
                swap[...], back[x, part, pl.ds(j * 8, 8)].reshape(SWAP, 128), preferred_element_type=F32
            )
            b_half[:, rows] = out.astype(BF16).reshape(8, EIGHTS, 128)
            return 0

        lax.fori_loop(0, 2, swap_in, 0)

        def combine(j, _, x=x, part=part):
            pair = jnp.concatenate((b_half[2 * j], b_half[2 * j + 1]), axis=1)
            both = jnp.dot(shares[x], pair, preferred_element_type=F32)
            both = both[0:128] + both[128:256]
            if x == 1:
                sums[part * 4 + j] = both
            else:
                cols = pl.ds(pl.multiple_of(part * 1024 + j * 256, 256), 256)
                expert_out[:, cols] = (sums[part * 4 + j] + both).astype(BF16)
            return 0

        lax.fori_loop(0, 4, combine, 0)
    for x in range(LOCAL):
        drain(slots.at[x, 0 : EP - 1], a_send.at[x])
        for part in range(2):
            drain(b_slots.at[x, part, 0 : EP - 1], b_send.at[x, part])
    for way in range(2):
        drain(wz.at[0:STEPS, 0:2], z_send.at[way])
        drain(units.at[0:STEPS, 0, 0], r_send.at[way])
        drain(units.at[:, 0, 0], c_send.at[way])
        for m in range(STEPS + 1 - C_OUT, STEPS + 1):
            help_copy(way, m).wait_send()
        for m in range(STEPS - R_OUT, STEPS + 1):
            sum_copy(way, m).wait_send()


def hand_out_kernel(mixer_in, expert_in, mixer_out, expert_out):
    mixer_out[...] = mixer_in[...]
    expert_out[...] = expert_in[...]


DMA = pltpu.SemaphoreType.DMA


def per_device(
    mixer_in, expert_in, mixer_gain, w_outer, w_inner, w_value, conv_taps, w_mix_out,
    expert_gain, w_gate, w_up, w_down, route_ids, route_weights,
):
    tok_count, width = expert_in.shape
    vmem = pl.BlockSpec(memory_space=pltpu.VMEM)
    anywhere = pl.BlockSpec(memory_space=pl.ANY)
    out = jax.ShapeDtypeStruct((tok_count, width), BF16)
    mixer_out, expert_out, _ = pl.pallas_call(
        whole_kernel,
        out_shape=(out, out, jax.ShapeDtypeStruct((EP, 2 * NZ, 4, 128, 128), BF16)),
        in_specs=[anywhere] * 14,
        out_specs=(vmem, vmem, anywhere),
        scratch_shapes=[
            pltpu.VMEM((tok_count, width), BF16),
            pltpu.VMEM((1, width), F32),
            pltpu.VMEM((1, width), F32),
            pltpu.VMEM((2, tok_count), jnp.int32),
            pltpu.VMEM((2, tok_count), F32),
            pltpu.VMEM((8, 128), F32),
            pltpu.VMEM((tok_count, width), BF16),
            pltpu.VMEM(w_down.shape, BF16),
            pltpu.VMEM((LOCAL, EP, EIGHTS, 256), BF16),
            pltpu.VMEM((LOCAL, EP, EIGHTS, 256), BF16),
            pltpu.VMEM((LOCAL, 2, EP, EIGHTS, 128), BF16),
            pltpu.VMEM((LOCAL, 2, EP, EIGHTS, 128), BF16),
            pltpu.VMEM((8, ROWS, 256), BF16),
            pltpu.VMEM((8, ROWS, 128), BF16),
            pltpu.VMEM((NZ, 4, 128, 128), BF16),
            pltpu.VMEM((16, width), BF16),
            pltpu.VMEM((tok_count + 16, width), BF16),
            pltpu.VMEM((NZ * 2, 8, 128), F32),
            pltpu.VMEM((NZ, 2, LOCAL, ROWS, width), BF16),
            pltpu.VMEM((LOCAL, width, 256), BF16),
            pltpu.VMEM((NZ, 2, LOCAL, ROWS, 128), BF16),
            pltpu.VMEM((2, C_OUT, ROWS, width), BF16),
            pltpu.VMEM((2, C_IN, ROWS, width), BF16),
            pltpu.VMEM((2, R_OUT, ROWS, width), BF16),
            pltpu.VMEM((2, STEPS, ROWS, width), BF16),
            pltpu.VMEM((SWAP, SWAP), BF16),
            pltpu.VMEM((LOCAL, 256, ROWS), BF16),
            pltpu.VMEM((8, 128, 256), F32),
            pltpu.VMEM((NZ * 2, 128, 128), BF16),
            pltpu.VMEM((2, EP, 3, 128, 128), BF16),
            DMA((1,)), DMA((1,)), DMA((LOCAL,)), DMA((LOCAL,)), DMA((LOCAL, 2)), DMA((LOCAL, 2)),
            DMA((2,)), DMA((2, STEPS)), DMA((1,)), DMA((1,)), DMA((2,)),
            DMA((2,)), DMA((2, STEPS)), DMA((2,)), DMA((2, STEPS + 1)),
            DMA((KINDS,)), DMA((KINDS,)), DMA((KINDS,)), DMA((KINDS,)), DMA((3,)),
            DMA((2, STEPS + 1)), DMA((2, STEPS + 1)), DMA((2, STEPS + 1)), DMA((2, STEPS + 1)),
            DMA((2, 2)), DMA((8,)),
            pltpu.SemaphoreType.REGULAR((2,)),
        ],
        cost_estimate=pl.CostEstimate(flops=10**11, bytes_accessed=3 * 10**8, transcendentals=0),
        compiler_params=pltpu.CompilerParams(
            collective_id=0, has_side_effects=True, vmem_limit_bytes=67043328
        ),
        name="whole_block",
    )(
        expert_in, mixer_gain[None, :], expert_gain[None, :], route_ids.T, route_weights.T, conv_taps,
        mixer_in, w_down, w_outer, w_inner, w_value, w_mix_out, w_gate, w_up,
    )
    return pl.pallas_call(
        hand_out_kernel,
        out_shape=(out, out),
        in_specs=[vmem, vmem],
        out_specs=(vmem, vmem),
        name="hand_out",
    )(mixer_out, expert_out)


def solution(mesh):
    finer = Mesh(mesh.devices.reshape(mesh.shape["ep"], 8, 2), EP_TP)
    return jax.shard_map(
        per_device,
        mesh=finer,
        in_specs=(
            P(EP_TP, None), P(EP_TP, None), P(), P(None, TP), P(None, TP), P(None, TP),
            P(None, TP), P(TP, None), P(), P("ep", None, TP), P("ep", None, TP),
            P("ep", TP, None), P(EP_TP, None), P(EP_TP, None),
        ),
        out_specs=(P(EP_TP, None), P(EP_TP, None)),
        check_vma=False,
    )
```

```python
import functools

import jax
import jax.numpy as jnp
from jax import lax
from jax.experimental import pallas as pl
from jax.experimental.pallas import tpu as pltpu
from jax.sharding import Mesh
from jax.sharding import PartitionSpec as P

EXPERTS = 32
CAP = 10
EIGHTS = 80
EP = 16
NZ = 8
LOCAL = 2
ROWS = EP * CAP
TP = ("tp_0", "tp_1")
EP_TP = ("ep", "tp_0", "tp_1")
MESH = pl.DeviceIdType.MESH
F32 = jnp.float32
BF16 = jnp.bfloat16

norm_eps = 1e-06
clamp_limit = 7.0
gate_alpha = 1.702


def normed(values, gain):
    scaled = values * lax.rsqrt(jnp.mean(values * values, axis=-1, keepdims=True) + norm_eps)
    return (scaled * gain).astype(BF16)


def places():
    return lax.axis_index("ep"), lax.axis_index("tp_0"), lax.axis_index("tp_1")


def signal(where):
    pl.semaphore_signal(
        pltpu.get_barrier_semaphore(), inc=1, device_id=where, device_id_type=MESH
    )


def signal_all(count, where):
    def one(k, _):
        signal(where(k))
        return 0

    lax.fori_loop(1, count, one, 0)


def signal_ring(ep, z, core):
    for step in (1, NZ - 1):
        signal((ep, lax.rem(z + step, NZ), core))
    signal((ep, z, 1 - core))


def remote(src, dst, send, recv, where):
    return pltpu.make_async_remote_copy(
        src_ref=src, dst_ref=dst, send_sem=send, recv_sem=recv, device_id=where, device_id_type=MESH
    )


def drain(ref, sem):
    pltpu.make_async_copy(ref, ref, sem).wait()


def each(count, act):
    def one(k, _):
        act(k)
        return 0

    lax.fori_loop(1, count, one, 0)


GATHER_D = (1, 1, 2, 2, 3, 3, 4)
GATHER_X = ((0, 1, 0, 1, 0, 1, 0), (0, 1, 0, 1, 0, 1, 1))
SCATTER_D = ((3, 4, 2, 3, 1, 2, 1), (3, 4, 3, 2, 2, 1, 1))
SCATTER_X = ((1, 0, 1, 0, 1, 0, 0), (0, 1, 1, 0, 1, 1, 0))
SCATTER_IN = ((None, None, 0, 1, 2, 3, 5), (None, None, 1, 0, 2, 4, 3))
LAST_IN = {(1, 0): (4, 5), (1, 1): (4, 5), (0, 0): (6, 6), (0, 1): (7, 7)}
STEPS = 7
C_IN = 3
SWAP = 8 * EIGHTS
C_OUT = 2
R_OUT = 3
LINE = (0, 3, 1, 2)
KINDS = 10


def forwards(way, n):
    nxt = 6 if (way, n) == (1, 5) else n + 2
    if nxt < STEPS and GATHER_X[way][nxt] == GATHER_X[way][n] and GATHER_D[nxt] == GATHER_D[n] + 1:
        return nxt
    return None


def whole_kernel(
    expert_hbm, mixer_gain_hbm, expert_gain_hbm, ids_hbm, weights_hbm, taps_hbm,
    mixer_hbm, down_hbm, w_outer, w_inner, w_value, w_mix, w_gate, w_up,
    mixer_out, expert_out, wall,
    expert_in, mixer_gain, expert_gain, ids, weights, tap, mixer_in, w_down,
    slots, landed, b_slots, back, b_in, b_half, wz, halo, mix_rows, taps_all, units, w_both, hid,
    c_out, c_in, r_out, r_in, swap, shares, sums, gated, w_slots,
    w_sem, g_sem, a_send, a_recv, b_send, b_recv, z_send, z_recv, t_send, t_recv, h_sem,
    r_send, r_recv, c_send, c_recv, x_send, x_recv, d_send, d_recv, o_sem,
    s_send, s_recv, p_send, p_recv, m_sem, i_sem, free_sem,
):
    ep, z, core = places()
    own = pl.ds(pl.multiple_of(ep * 128, 128), 128)
    for i, w in enumerate((w_inner, w_value, w_outer)):
        pltpu.make_async_copy(w.at[own], wz.at[z, i], w_sem.at[0]).start()
    pltpu.make_async_copy(w_mix.at[:, own], wz.at[z, 3], w_sem.at[0]).start()
    pairs = (
        (expert_hbm, expert_in), (expert_gain_hbm, expert_gain), (ids_hbm, ids),
        (weights_hbm, weights), (taps_hbm, tap.at[0:3]), (mixer_gain_hbm, mixer_gain),
        (mixer_hbm, mixer_in), (down_hbm, w_down),
    )
    inputs = [pltpu.make_async_copy(src, dst, i_sem.at[i]) for i, (src, dst) in enumerate(pairs)]
    for load in inputs:
        load.start()
    for x in range(LOCAL):
        pltpu.make_async_copy(w_gate.at[x], w_both.at[x, :, 0:128], g_sem.at[0]).start()
        pltpu.make_async_copy(w_up.at[x], w_both.at[x, :, 128:256], g_sem.at[0]).start()
    spot = z * 2 + core
    partner = (ep, z, 1 - core)

    def tp_peer(k):
        to = lax.rem(spot + k, NZ * 2)
        return ep, to // 2, lax.rem(to, 2)

    def in_order(step):
        to = lax.rem(ep * (NZ * 2) + spot + step, EP * NZ * 2)
        return to // (NZ * 2), lax.rem(to // 2, NZ), lax.rem(to, 2)

    def ep_peer(k):
        return lax.rem(ep + k, EP), z, core

    signal_all(EP, ep_peer)
    signal_all(NZ * 2, tp_peer)
    signal(in_order(1))
    signal(in_order(EP * NZ * 2 - 1))

    def exchange(x, k):
        where = ep_peer(k)
        return remote(
            slots.at[x, where[0]], landed.at[x, ep], a_send.at[x], a_recv.at[x], where
        )

    def hand_back(x, part, k):
        where = ep_peer(k)
        return remote(
            b_slots.at[x, part, where[0]], back.at[x, part, ep],
            b_send.at[x, part], b_recv.at[x, part], where,
        )

    def tell_taps(k):
        return remote(tap, taps_all.at[spot], t_send.at[0], t_recv.at[0], tp_peer(k))

    def tell_tail():
        return remote(mix_rows.at[128:144], halo, h_sem.at[0], h_sem.at[1], in_order(1))

    steps = (NZ - 1, 1)

    def spread_z(way, n):
        hops = 2 if n == STEPS - 1 else 1
        at = lax.rem(z + (GATHER_D[n] - hops) * steps[way], NZ)
        there = (ep, lax.rem(z + hops * (NZ - steps[way]), NZ), core)
        two = pl.ds(2 * GATHER_X[way][n], 2)
        return remote(
            wz.at[at, two], wz.at[at, two], z_send.at[way], z_recv.at[way, n], there
        )

    def ring_copy(way, n):
        at = lax.rem(z + (GATHER_D[n] - 1) * steps[way], NZ)
        x = GATHER_X[way][n]
        there = lax.rem(z + (NZ - steps[way]), NZ)
        ref = units.at[at, core, x]
        return remote(ref, ref, r_send.at[way], r_recv.at[way, n], (ep, there, core))

    def across(way, n):
        mine = n == STEPS
        at = z if mine else lax.rem(z + GATHER_D[n] * steps[way], NZ)
        x = way if mine else GATHER_X[way][n]
        ref = units.at[at, core, x]
        return remote(ref, ref, c_send.at[way], c_recv.at[way, n], partner), at, x

    at_x, at_y = lax.rem(ep, 4), ep // 4

    def off(half, du, dv):
        dx, dy = (du, dv) if half == 0 else (dv, du)
        return lax.rem(at_y + dy, 4) * 4 + lax.rem(at_x + dx, 4)

    def piece(half, way, kind, e, at_core):
        zs = pl.ds(at_core * NZ + 4 * half, 4)
        if kind == 1 or kind >= 6:
            zs = pl.ds(at_core * NZ + 4 * half + 2 * way, 2)
        return wall.at[e, zs]

    def plane(half, way, kind):
        step = 1 if way == 0 else 3
        if kind == 0:
            e, to = ep, off(half, step, 0)
        elif kind == 1:
            e, to = off(half, 4 - step, 0), off(half, step, 0)
        elif kind < 6:
            e, to = off(half, LINE[kind - 2], 0), off(half, 0, step)
        else:
            e, to = off(half, LINE[kind - 6], 4 - step), off(half, 0, step)
        ref = piece(half, way, kind, e, core)
        return remote(
            wz.at[pl.ds(4 * half, 4)] if kind in (0, 2) else ref, ref,
            x_send.at[kind], x_recv.at[kind], (to, z, core),
        )

    def plane_over(half, way, kind):
        step = 1 if way == 0 else 3
        if kind == 0:
            e = off(half, 4 - step, 0)
        elif kind == 1:
            e = off(half, 2, 0)
        elif kind < 6:
            e = off(half, LINE[kind - 2], 4 - step)
        else:
            e = off(half, LINE[kind - 6], 2)
        ref = piece(half, way, kind, e, core)
        return remote(ref, ref, d_send.at[kind], d_recv.at[kind], partner)

    both_halves = [(half, way) for half in range(2) for way in range(2)]

    def four(kind):
        return wall.at[0, 0 : (NZ if kind == 1 or kind >= 6 else 2 * NZ)]

    def take(*kinds):
        for kind in kinds:
            drain(four(kind), x_recv.at[kind])
            for half, way in both_halves:
                plane_over(half, way, kind).start()

    def give(*kinds):
        for kind in kinds:
            for half, way in both_halves:
                plane(half, way, kind).start()

    own_wall = wall.at[ep, pl.ds(core * NZ, NZ)]

    def own_over():
        return remote(wz, own_wall, o_sem.at[0], o_sem.at[1], partner)

    def own_keep():
        return pltpu.make_async_copy(wz, own_wall, o_sem.at[2])

    def compute(at_z, at_core, x):
        both = jnp.dot(units[at_z, at_core, x], w_both[x], preferred_element_type=F32)
        gate_pre = jnp.minimum(both[:, 0:128], clamp_limit)
        up_pre = jnp.clip(both[:, 128:256], -clamp_limit, clamp_limit)
        hid[at_z, at_core, x] = (
            (up_pre + 1.0) * gate_pre * jax.nn.sigmoid(gate_alpha * gate_pre)
        ).astype(BF16)

    def pass_z(n):
        for way in range(2):
            spread_z(way, n).wait_recv()
            for nxt in (n + 2, STEPS - 1):
                hops = 2 if nxt == STEPS - 1 else 1
                if nxt < STEPS and nxt > n and (nxt == n + 2 or n in (2, 3)):
                    if (GATHER_X[way][nxt], GATHER_D[nxt]) == (GATHER_X[way][n], GATHER_D[n] + hops):
                        spread_z(way, nxt).start()

    go = (1, NZ - 1)

    def place(way, m):
        if m == STEPS:
            return z, way
        return lax.rem(z + SCATTER_D[way][m] * go[way], NZ), SCATTER_X[way][m]

    def help_copy(way, m):
        return remote(
            c_out.at[way, m % C_OUT], c_in.at[way, m % C_IN], p_send.at[way, m], p_recv.at[way, m], partner
        )

    def sum_copy(way, m):
        cols = slice(0, 2048) if m < 6 else slice(1024 * (m - 6), 1024 * (m - 5))
        step = min(m, 6)
        return remote(
            r_out.at[way, step % R_OUT, :, cols], r_in.at[way, step, :, cols],
            s_send.at[way, m], s_recv.at[way, m], (ep, lax.rem(z + go[way], NZ), core),
        )

    def partial(at, at_core, x, add, out, tiles=(0, 4)):
        def tile(j, _):
            cols = pl.ds(pl.multiple_of(j * 512, 512), 512)
            total = jnp.dot(hid[at, at_core, x], w_down[x, :, cols], preferred_element_type=F32)
            for ref in add:
                total = total + ref[:, cols].astype(F32)
            out[:, cols] = total.astype(BF16)
            return 0

        lax.fori_loop(*tiles, tile, 0)

    def help_other(m):
        for way in range(2):
            at, x = place(way, m)
            if m >= C_OUT:
                help_copy(way, m - C_OUT).wait_send()
            partial(at, 1 - core, x, (), c_out.at[way, m % C_OUT])
            if m >= C_IN:
                pl.semaphore_wait(free_sem.at[way], 1)
            help_copy(way, m).start()

    def used(way, m):
        if m + C_IN <= STEPS:
            pl.semaphore_signal(free_sem.at[way], inc=1, device_id=partner, device_id_type=MESH)

    def send_sum(way, m):
        at, x = place(way, m)
        add = [c_in.at[way, m % C_IN]]
        help_copy(way, m).wait_recv()
        came = SCATTER_IN[way][m]
        if came is not None:
            sum_copy(way, came).wait_recv()
            add.append(r_in.at[way, came])
        if m >= R_OUT:
            sum_copy(way, m - R_OUT).wait_send()
        if m < 6:
            partial(at, core, x, add, r_out.at[way, m % R_OUT])
            sum_copy(way, m).start()
        else:
            for part in range(2):
                partial(at, core, x, add, r_out.at[way, m % R_OUT], (2 * part, 2 * part + 2))
                sum_copy(way, 6 + part).start()
        used(way, m)

    def fetch(t):
        at = lax.rem(t, 2)
        return pltpu.make_async_copy(wall.at[:, t, 0:3], w_slots.at[at], m_sem.at[at, 0])

    def fetch_last(j):
        at = lax.rem(j, 2)
        return [
            pltpu.make_async_copy(wall.at[2 * j + i, :, 3], w_slots.at[at, :, i], m_sem.at[at, i])
            for i in range(2)
        ]

    def mix(t, _):
        fetch(t).wait()
        at = lax.rem(t, 2)
        rows = mix_rows[...]
        pair = jnp.concatenate([w_slots[at, :, i].reshape(2048, 128) for i in range(2)], axis=1)
        pair = jnp.dot(rows, pair, preferred_element_type=F32)
        prod = pair[:, 0:128] * pair[:, 128:256]
        outer = jnp.dot(
            rows[16:144], w_slots[at, :, 2].reshape(2048, 128), preferred_element_type=F32
        )
        tap_at = taps_all[lax.rem(t, NZ) * 2 + t // NZ]
        conv = tap_at[2:3] * prod[16:144] + tap_at[1:2] * prod[15:143] + tap_at[0:1] * prod[14:142]
        gated[t] = (outer * conv).astype(BF16)

        @pl.when(t + 2 < NZ * 2)
        def _():
            fetch(t + 2).start()

        return 0

    def last(j, _):
        for copy in fetch_last(j):
            copy.wait()
        at = lax.rem(j, 2)
        rows = jnp.concatenate([gated[t] for t in range(NZ * 2)], axis=1)
        pair = jnp.concatenate([w_slots[at, :, i].reshape(2048, 128) for i in range(2)], axis=1)
        cols = pl.ds(pl.multiple_of(j * 256, 256), 256)
        mixer_out[:, cols] = jnp.dot(rows, pair, preferred_element_type=F32).astype(BF16)

        @pl.when(j + 2 < EP // 2)
        def _():
            for copy in fetch_last(j + 2):
                copy.start()

        return 0

    def fill_swap(j, _):
        rows = pl.ds(pl.multiple_of(j * 320, 320), 320)
        row = lax.broadcasted_iota(jnp.int32, (320, 1), 0) + j * 320
        col = lax.broadcasted_iota(jnp.int32, (320, SWAP), 1)
        to = lax.rem(row, EIGHTS) // CAP * EIGHTS + row // EIGHTS * CAP + lax.rem(row, CAP)
        swap[rows] = (to == col).astype(F32).astype(BF16)
        return 0

    def spread_rows(x):
        def one(j, _):
            rows = pl.ds(pl.multiple_of(j * EIGHTS, EIGHTS), EIGHTS)
            wide = jnp.dot(swap[...], b_in[:, rows].reshape(SWAP, 256), preferred_element_type=F32)
            slots[x, pl.ds(j * 8, 8)] = wide.astype(BF16).reshape(8, EIGHTS, 256)
            return 0

        lax.fori_loop(0, 2, one, 0)

    def gather_rows(got):
        def one(j, _):
            rows = pl.ds(pl.multiple_of(j * EIGHTS, EIGHTS), EIGHTS)
            out = jnp.dot(swap[...], got[pl.ds(j * 8, 8)].reshape(SWAP, 256), preferred_element_type=F32)
            b_in[:, rows] = out.astype(BF16).reshape(8, EIGHTS, 256)
            return 0

        lax.fori_loop(0, 2, one, 0)

    tap[3:8] = jnp.zeros((5, 128), F32)
    lax.fori_loop(0, 2, fill_swap, 0)
    for load in inputs[0:3]:
        load.wait()
    rows = normed(expert_in[...].astype(F32), expert_gain[...])
    experts = lax.broadcasted_iota(jnp.int32, (EXPERTS, 128), 0)
    hits = [experts == ids[k : k + 1, :] for k in range(2)]
    member = (hits[0] | hits[1]).astype(F32).astype(BF16)
    before = lax.broadcasted_iota(jnp.int32, (128, 128), 0) < lax.broadcasted_iota(jnp.int32, (128, 128), 1)
    earlier = jnp.dot(member, before.astype(F32).astype(BF16), preferred_element_type=F32)
    goes = []
    for k in range(2):
        slot = jnp.sum(jnp.where(hits[k], earlier, 0.0), axis=0, keepdims=True).astype(jnp.int32)
        one = ids[k : k + 1, :]
        goes.append((one & 1) * ROWS + (one >> 1) * CAP + slot)
    slot_row = lax.broadcasted_iota(jnp.int32, (ROWS, 128), 0)

    def fill_slots(x):
        placing = (slot_row + x * ROWS == goes[0]) | (slot_row + x * ROWS == goes[1])
        out = jnp.dot(placing.astype(F32).astype(BF16), rows, preferred_element_type=F32).astype(BF16)
        for j in range(8):
            b_in[j] = out[:, j * 256 : (j + 1) * 256]
        spread_rows(x)

    fill_slots(0)
    pl.semaphore_wait(pltpu.get_barrier_semaphore(), EP + NZ * 2)
    drain(wz.at[z], w_sem.at[0])
    for n in range(LOCAL):
        for way in range(2):
            spread_z(way, n).start()
    each(EP, lambda k: exchange(0, k).start())
    pass_z(0)
    fill_slots(1)
    each(EP, lambda k: exchange(1, k).start())
    pass_z(1)
    for x in range(LOCAL):
        landed[x, ep] = slots[x, ep]
    for load in inputs[3:]:
        load.wait()
    each(NZ * 2, lambda k: tell_taps(k).start())
    mixed = normed(mixer_in[...].astype(F32), mixer_gain[...])
    mix_rows[16:144] = mixed
    pass_z(2)
    tell_tail().start()
    taps_all[spot] = tap[...]
    slot_row = lax.broadcasted_iota(jnp.int32, (LOCAL * ROWS, 128), 0)
    held = jnp.zeros((LOCAL * ROWS, 128), F32)
    for k in range(2):
        held = held + jnp.where(slot_row == goes[k], weights[k : k + 1, :], 0.0)
    pass_z(3)
    for x in range(LOCAL):
        total = held[x * ROWS : (x + 1) * ROWS].T
        high = total.astype(BF16)
        shares[x, 0:128] = high
        shares[x, 128:256] = (total - high.astype(F32)).astype(BF16)
    drain(w_both, g_sem.at[0])

    def pack(x):
        drain(landed.at[x, 0 : EP - 1], a_recv.at[x])
        gather_rows(landed.at[x])
        for j in range(8):
            units[z, core, x, :, j * 256 : (j + 1) * 256] = b_in[j]
        for way in range(2):
            ring_copy(way, x).start()
        across(x, STEPS)[0].start()

    pack(0)
    compute(z, core, 0)
    pack(1)
    for n in range(4, STEPS):
        pass_z(n)
    give(0)
    give(2)
    own_over().start()
    own_keep().start()
    compute(z, core, 1)
    tell_tail().wait()
    lone = (ep == 0) & (spot == 0)
    mix_rows[0:16] = jnp.where(lone, jnp.zeros_like(halo), halo[...])
    drain(taps_all.at[0 : NZ * 2 - 1], t_recv.at[0])
    drain(taps_all.at[0 : NZ * 2 - 1], t_send.at[0])
    for x in range(LOCAL):
        copy, at, _ = across(x, STEPS)
        copy.wait_recv()
        compute(z, 1 - core, x)

    for n in range(STEPS):
        for way in range(2):
            ring_copy(way, n).wait_recv()
            nxt = forwards(way, n)
            if nxt is not None:
                ring_copy(way, nxt).start()
            across(way, n)[0].start()
        if n == 1:
            take(0)
            give(1, 3, 4)
        elif n == 2:
            take(2)
            give(6)
            take(1)
            give(5)
        elif n == 3:
            take(3)
            give(7)
        elif n == 4:
            take(4)
            give(8)
            take(6)
        for way in range(2):
            at = lax.rem(z + GATHER_D[n] * steps[way], NZ)
            compute(at, core, GATHER_X[way][n])
        for way in range(2):
            copy, at, x = across(way, n)
            copy.wait_recv()
            compute(at, 1 - core, x)
        if n == 5:
            help_other(0)
            send_sum(1, 0)
            send_sum(0, 0)
            take(5)
            give(9)
        elif n == 6:
            help_other(1)
            send_sum(0, 1)
            send_sum(1, 1)
            help_other(2)
            take(7, 8)
    take(9)
    own_keep().wait()
    own_over().wait()
    for kind in range(KINDS):
        for sem in (d_recv, d_send, x_send):
            drain(four(kind), sem.at[kind])
    fetch(0).start()
    fetch(1).start()
    send_sum(0, 2)
    lax.fori_loop(0, 6, mix, 0)
    help_other(3)
    send_sum(1, 2)
    send_sum(0, 3)
    send_sum(1, 3)
    help_other(4)
    lax.fori_loop(6, 11, mix, 0)
    send_sum(0, 4)
    send_sum(1, 4)
    help_other(5)
    lax.fori_loop(11, NZ * 2, mix, 0)
    for j in range(2):
        for copy in fetch_last(j):
            copy.start()
    send_sum(0, 5)
    help_other(6)
    lax.fori_loop(0, EP // 2, last, 0)
    send_sum(1, 5)
    send_sum(0, 6)
    send_sum(1, 6)
    help_other(7)

    for x, part in ((1, 0), (1, 1), (0, 0), (0, 1)):
        if part == 0:
            help_copy(x, STEPS).wait_recv()
        if part == 0 or x == 0:
            for way in range(2):
                sum_copy(way, LAST_IN[x, part][way]).wait_recv()

        def tile(j, _, x=x, part=part):
            cols = pl.ds(pl.multiple_of(part * 1024 + j * 256, 256), 256)
            total = jnp.dot(hid[z, core, x], w_down[x, :, cols], preferred_element_type=F32)
            for ref in (
                c_in.at[x, STEPS % C_IN],
                r_in.at[0, min(LAST_IN[x, part][0], 6)],
                r_in.at[1, min(LAST_IN[x, part][1], 6)],
            ):
                total = total + ref[:, cols].astype(F32)
            total = total.astype(BF16)
            b_half[2 * j] = total[:, 0:128]
            b_half[2 * j + 1] = total[:, 128:256]
            return 0

        lax.fori_loop(0, 4, tile, 0)

        def swap_out(j, _, x=x, part=part):
            rows = pl.ds(pl.multiple_of(j * EIGHTS, EIGHTS), EIGHTS)
            wide = jnp.dot(swap[...], b_half[:, rows].reshape(SWAP, 128), preferred_element_type=F32)
            b_slots[x, part, pl.ds(j * 8, 8)] = wide.astype(BF16).reshape(8, EIGHTS, 128)
            return 0

        lax.fori_loop(0, 2, swap_out, 0)
        each(EP, lambda k, x=x, part=part: hand_back(x, part, k).start())
        back[x, part, ep] = b_slots[x, part, ep]

    for x, part in ((1, 0), (1, 1), (0, 0), (0, 1)):
        drain(back.at[x, part, 0 : EP - 1], b_recv.at[x, part])

        def swap_in(j, _, x=x, part=part):
            rows = pl.ds(pl.multiple_of(j * EIGHTS, EIGHTS), EIGHTS)
            out = jnp.dot(
                swap[...], back[x, part, pl.ds(j * 8, 8)].reshape(SWAP, 128), preferred_element_type=F32
            )
            b_half[:, rows] = out.astype(BF16).reshape(8, EIGHTS, 128)
            return 0

        lax.fori_loop(0, 2, swap_in, 0)

        def combine(j, _, x=x, part=part):
            pair = jnp.concatenate((b_half[2 * j], b_half[2 * j + 1]), axis=1)
            both = jnp.dot(shares[x], pair, preferred_element_type=F32)
            both = both[0:128] + both[128:256]
            if x == 1:
                sums[part * 4 + j] = both
            else:
                cols = pl.ds(pl.multiple_of(part * 1024 + j * 256, 256), 256)
                expert_out[:, cols] = (sums[part * 4 + j] + both).astype(BF16)
            return 0

        lax.fori_loop(0, 4, combine, 0)
    for x in range(LOCAL):
        drain(slots.at[x, 0 : EP - 1], a_send.at[x])
        for part in range(2):
            drain(b_slots.at[x, part, 0 : EP - 1], b_send.at[x, part])
    for way in range(2):
        drain(wz.at[0:STEPS, 0:2], z_send.at[way])
        drain(units.at[0:STEPS, 0, 0], r_send.at[way])
        drain(units.at[:, 0, 0], c_send.at[way])
        for m in range(STEPS + 1 - C_OUT, STEPS + 1):
            help_copy(way, m).wait_send()
        for m in range(STEPS - R_OUT, STEPS + 1):
            sum_copy(way, m).wait_send()


def hand_out_kernel(mixer_in, expert_in, mixer_out, expert_out):
    mixer_out[...] = mixer_in[...]
    expert_out[...] = expert_in[...]


DMA = pltpu.SemaphoreType.DMA


def per_device(
    mixer_in, expert_in, mixer_gain, w_outer, w_inner, w_value, conv_taps, w_mix_out,
    expert_gain, w_gate, w_up, w_down, route_ids, route_weights,
):
    tok_count, width = expert_in.shape
    vmem = pl.BlockSpec(memory_space=pltpu.VMEM)
    anywhere = pl.BlockSpec(memory_space=pl.ANY)
    out = jax.ShapeDtypeStruct((tok_count, width), BF16)
    mixer_out, expert_out, _ = pl.pallas_call(
        whole_kernel,
        out_shape=(out, out, jax.ShapeDtypeStruct((EP, 2 * NZ, 4, 128, 128), BF16)),
        in_specs=[anywhere] * 14,
        out_specs=(vmem, vmem, anywhere),
        scratch_shapes=[
            pltpu.VMEM((tok_count, width), BF16),
            pltpu.VMEM((1, width), F32),
            pltpu.VMEM((1, width), F32),
            pltpu.VMEM((2, tok_count), jnp.int32),
            pltpu.VMEM((2, tok_count), F32),
            pltpu.VMEM((8, 128), F32),
            pltpu.VMEM((tok_count, width), BF16),
            pltpu.VMEM(w_down.shape, BF16),
            pltpu.VMEM((LOCAL, EP, EIGHTS, 256), BF16),
            pltpu.VMEM((LOCAL, EP, EIGHTS, 256), BF16),
            pltpu.VMEM((LOCAL, 2, EP, EIGHTS, 128), BF16),
            pltpu.VMEM((LOCAL, 2, EP, EIGHTS, 128), BF16),
            pltpu.VMEM((8, ROWS, 256), BF16),
            pltpu.VMEM((8, ROWS, 128), BF16),
            pltpu.VMEM((NZ, 4, 128, 128), BF16),
            pltpu.VMEM((16, width), BF16),
            pltpu.VMEM((tok_count + 16, width), BF16),
            pltpu.VMEM((NZ * 2, 8, 128), F32),
            pltpu.VMEM((NZ, 2, LOCAL, ROWS, width), BF16),
            pltpu.VMEM((LOCAL, width, 256), BF16),
            pltpu.VMEM((NZ, 2, LOCAL, ROWS, 128), BF16),
            pltpu.VMEM((2, C_OUT, ROWS, width), BF16),
            pltpu.VMEM((2, C_IN, ROWS, width), BF16),
            pltpu.VMEM((2, R_OUT, ROWS, width), BF16),
            pltpu.VMEM((2, STEPS, ROWS, width), BF16),
            pltpu.VMEM((SWAP, SWAP), BF16),
            pltpu.VMEM((LOCAL, 256, ROWS), BF16),
            pltpu.VMEM((8, 128, 256), F32),
            pltpu.VMEM((NZ * 2, 128, 128), BF16),
            pltpu.VMEM((2, EP, 3, 128, 128), BF16),
            DMA((1,)), DMA((1,)), DMA((LOCAL,)), DMA((LOCAL,)), DMA((LOCAL, 2)), DMA((LOCAL, 2)),
            DMA((2,)), DMA((2, STEPS)), DMA((1,)), DMA((1,)), DMA((2,)),
            DMA((2,)), DMA((2, STEPS)), DMA((2,)), DMA((2, STEPS + 1)),
            DMA((KINDS,)), DMA((KINDS,)), DMA((KINDS,)), DMA((KINDS,)), DMA((3,)),
            DMA((2, STEPS + 1)), DMA((2, STEPS + 1)), DMA((2, STEPS + 1)), DMA((2, STEPS + 1)),
            DMA((2, 2)), DMA((8,)),
            pltpu.SemaphoreType.REGULAR((2,)),
        ],
        cost_estimate=pl.CostEstimate(flops=10**11, bytes_accessed=3 * 10**8, transcendentals=0),
        compiler_params=pltpu.CompilerParams(
            collective_id=0, has_side_effects=True, vmem_limit_bytes=67043328
        ),
        name="whole_block",
    )(
        expert_in, mixer_gain[None, :], expert_gain[None, :], route_ids.T, route_weights.T, conv_taps,
        mixer_in, w_down, w_outer, w_inner, w_value, w_mix_out, w_gate, w_up,
    )
    return pl.pallas_call(
        hand_out_kernel,
        out_shape=(out, out),
        in_specs=[vmem, vmem],
        out_specs=(vmem, vmem),
        name="hand_out",
    )(mixer_out, expert_out)


def solution(mesh):
    finer = Mesh(mesh.devices.reshape(mesh.shape["ep"], 8, 2), EP_TP)
    return jax.shard_map(
        per_device,
        mesh=finer,
        in_specs=(
            P(EP_TP, None), P(EP_TP, None), P(), P(None, TP), P(None, TP), P(None, TP),
            P(None, TP), P(TP, None), P(), P("ep", None, TP), P("ep", None, TP),
            P("ep", TP, None), P(EP_TP, None), P(EP_TP, None),
        ),
        out_specs=(P(EP_TP, None), P(EP_TP, None)),
        check_vma=False,
    )
```
